512 devices in a mesh: sp: 64 (over z, y), tp: 8 (over x, core).
Axes of the slice: x: 4, y: 8, z: 8, core: 2. Of those that a mesh axis runs over, the one named last changes fastest.
Arguments:
- residual: bfloat16 [8192, 2048], P(('sp', 'tp')), may hold values from -6 to 6
- q_small: bfloat16 [8192, 1024], P('sp', 'tp'), may hold values from -6 to 6
- k_small: bfloat16 [8192, 1024], P('sp', 'tp'), may hold values from -6 to 6
- v_small: bfloat16 [8192, 1024], P('sp', 'tp'), may hold values from -6 to 6
- q_large: bfloat16 [8192, 1024], P('sp', 'tp'), may hold values from -6 to 6
- k_large: bfloat16 [8192, 1024], P('sp', 'tp'), may hold values from -6 to 6
- v_large: bfloat16 [8192, 1024], P('sp', 'tp'), may hold values from -6 to 6
- forget_small: float32 [8192, 16], P('sp', 'tp'), may hold values from 0 to 20
- forget_large: float32 [8192, 8], P('sp', 'tp'), may hold values from 0 to 20
- w_out_small: bfloat16 [1024, 2048], P('tp'), may hold values from -0.125 to 0.125
- w_out_large: bfloat16 [1024, 2048], P('tp'), may hold values from -0.125 to 0.125
- norm_gain: float32 [2048], replicated, may hold values from 0.1 to 1.9
- w_gate: bfloat16 [2048, 4096], P('sp', 'tp'), may hold values from -0.125 to 0.125
- w_up: bfloat16 [2048, 4096], P('sp', 'tp'), may hold values from -0.125 to 0.125
- conv_gate: float32 [3, 4096], P(None, 'tp'), may hold values from -3 to 3
- conv_up: float32 [3, 4096], P(None, 'tp'), may hold values from -3 to 3
- w_down: bfloat16 [4096, 2048], P('tp', 'sp'), may hold values from -0.09375 to 0.09375
Outputs:
- mixed: bfloat16 [8192, 2048], P(('sp', 'tp'))
The draws below stay inside these ranges and needn't reach their ends.
All inputs are finite; a program needn't handle non-finite values.
Results may differ from the reference program's by a relative error of at most 0.015.
Values may be sent and summed in bfloat16 or wider, within the bound.
A program may use at most 64 MiB of HBM per device.

```python
import math
import jax
import jax.numpy as jnp
from jax import lax

D = 2048
FF = 4096
HEADS_SMALL = 16
HEAD_SMALL = 64
HEADS_LARGE = 8
HEAD_LARGE = 128
TOK_DEV = 128
TOKENS = 8192


def draw_planted(key, salt, heads, size, phase):
    base = jnp.clip(jax.random.normal(jax.random.fold_in(key, salt), (TOKENS, heads * size), jnp.float32), -6.0, 6.0)
    return base.astype(jnp.bfloat16)


def draw_gates(key, salt, heads):
    order = jax.random.permutation(jax.random.fold_in(key, salt), heads)
    fast_count = heads // 2
    fast = order < fast_count
    level = jnp.where(fast, 4.0, math.log(TOKENS) + 1.0)
    noise = jnp.clip(jax.random.normal(jax.random.fold_in(key, salt + 1), (TOKENS, heads), jnp.float32), -3.0, 3.0)
    blocks = jax.random.uniform(jax.random.fold_in(key, salt + 2), (TOKENS // TOK_DEV, heads), jnp.float32, -0.7, 0.7)
    return (level[None, :] + noise + jnp.repeat(blocks, TOK_DEV, axis=0)).astype(jnp.float32)


def draw_q_small(key, part):
    return draw_planted(key, 11, HEADS_SMALL, HEAD_SMALL, 40)


def draw_k_small(key, part):
    return draw_planted(key, 12, HEADS_SMALL, HEAD_SMALL, 3)


def draw_q_large(key, part):
    return draw_planted(key, 13, HEADS_LARGE, HEAD_LARGE, 40)


def draw_k_large(key, part):
    return draw_planted(key, 14, HEADS_LARGE, HEAD_LARGE, 3)


def draw_forget_small(key, part):
    return draw_gates(key, 21, HEADS_SMALL)


def draw_forget_large(key, part):
    return draw_gates(key, 31, HEADS_LARGE)


def level_of(key, extent, cuts, least, high):
    level, own = 1.0, jax.random.fold_in(key, 6)
    for position, shards_of in cuts:
        draws = jnp.exp(jax.random.uniform(jax.random.fold_in(own, position), (shards_of,), jnp.float32, least / len(cuts), high / len(cuts)))
        level = level * jnp.repeat(draws, extent[position] // shards_of).reshape([-1 if axis == position else 1 for axis in range(len(extent))])
    return level


def bell_draw(stream_key, extent, deviation, bound, cuts=(), kind=jnp.bfloat16):
    values = jax.random.normal(stream_key, extent, jnp.float32) * deviation
    if len(cuts) > 0:
        values = level_of(stream_key, extent, cuts, -0.22, 0.18) * values
    return jnp.clip(values, min=-bound, max=bound).astype(kind)


def setup_inputs(seed: int = 0) -> dict:
    key_of = jax.random.split(jax.random.key(seed), 18)
    return {
        "residual": bell_draw(key_of[0], (TOKENS, D), 1.0, 6.0, ((0, 512),)),
        "q_small": draw_q_small(jax.random.fold_in(key_of[17], 71), 0),
        "k_small": draw_k_small(jax.random.fold_in(key_of[17], 71), 0),
        "v_small": bell_draw(key_of[3], (TOKENS, HEADS_SMALL * HEAD_SMALL), 1.0, 6.0, ((0, 64), (1, 8))),
        "q_large": draw_q_large(jax.random.fold_in(key_of[17], 71), 0),
        "k_large": draw_k_large(jax.random.fold_in(key_of[17], 71), 0),
        "v_large": bell_draw(key_of[6], (TOKENS, HEADS_LARGE * HEAD_LARGE), 1.0, 6.0, ((0, 64), (1, 8))),
        "forget_small": draw_forget_small(jax.random.fold_in(key_of[17], 71), 0),
        "forget_large": draw_forget_large(jax.random.fold_in(key_of[17], 71), 0),
        "w_out_small": bell_draw(key_of[9], (HEADS_SMALL * HEAD_SMALL, D), (HEADS_SMALL * HEAD_SMALL + HEADS_LARGE * HEAD_LARGE) ** -0.5, 0.125, ((0, 8),)),
        "w_out_large": bell_draw(key_of[10], (HEADS_LARGE * HEAD_LARGE, D), (HEADS_SMALL * HEAD_SMALL + HEADS_LARGE * HEAD_LARGE) ** -0.5, 0.125, ((0, 8),)),
        "norm_gain": jnp.clip(1.0 + 0.18 * jax.random.normal(key_of[11], (D,), jnp.float32), 0.1, 1.9),
        "w_gate": bell_draw(key_of[12], (D, FF), D ** -0.5, 0.125, ((0, 64), (1, 8))),
        "w_up": bell_draw(key_of[13], (D, FF), D ** -0.5, 0.125, ((0, 64), (1, 8))),
        "conv_gate": bell_draw(key_of[14], (3, FF), 0.577, 3.0, ((1, 8),), jnp.float32),
        "conv_up": bell_draw(key_of[15], (3, FF), 0.577, 3.0, ((1, 8),), jnp.float32),
        "w_down": bell_draw(key_of[16], (FF, D), FF ** -0.5, 0.09375, ((0, 8), (1, 64))),
    }


EPS = 1e-06
NEG = -1e+30

def group_attention(queries, keys, values, forget, heads, size):
    total = queries.shape[0]
    cumul = jnp.cumsum(jax.nn.log_sigmoid(forget.astype(jnp.float32)), axis=0)
    qf = queries.reshape(total, heads, size).astype(jnp.float32)
    kf = keys.reshape(total, heads, size).astype(jnp.float32)
    vf = values.reshape(total, heads, size).astype(jnp.float32)
    block = math.gcd(total, 128)
    kpos = jnp.arange(total, dtype=jnp.int32)
    scale = size ** (-0.5)

    def one_block(start):
        qb = lax.dynamic_slice_in_dim(qf, start, block, 0)
        cb = lax.dynamic_slice_in_dim(cumul, start, block, 0)
        qpos = start + jnp.arange(block, dtype=jnp.int32)
        scores = jnp.einsum('qhd,khd->qhk', qb, kf) * scale + cb[:, :, None] - cumul.T[None, :, :]
        keep = (kpos[None, :] <= qpos[:, None])[:, None, :]
        scores = jnp.where(keep, scores, NEG)
        top = lax.optimization_barrier(jnp.max(scores, axis=-1, keepdims=True))
        weights = jnp.where(keep, jnp.exp(scores - top), 0.0)
        denom = lax.optimization_barrier(jnp.sum(weights, axis=-1))
        wbf = weights.astype(jnp.bfloat16).astype(jnp.float32)
        attended = jnp.einsum('qhk,khd->qhd', wbf, vf) / denom[:, :, None]
        normed = attended * lax.rsqrt(lax.optimization_barrier(jnp.mean(attended * attended, axis=-1, keepdims=True)) + EPS)
        return normed.astype(jnp.bfloat16).reshape(block, heads * size)
    starts = (jnp.arange(total // block) * block).astype(jnp.int32)
    return lax.map(one_block, starts).reshape(total, heads * size)

def reference(residual, q_small, k_small, v_small, q_large, k_large, v_large, forget_small, forget_large, w_out_small, w_out_large, norm_gain, w_gate, w_up, conv_gate, conv_up, w_down):
    normed_small = group_attention(q_small, k_small, v_small, forget_small, HEADS_SMALL, HEAD_SMALL)
    normed_large = group_attention(q_large, k_large, v_large, forget_large, HEADS_LARGE, HEAD_LARGE)
    first = residual.astype(jnp.float32) + jnp.dot(normed_small, w_out_small, preferred_element_type=jnp.float32) + jnp.dot(normed_large, w_out_large, preferred_element_type=jnp.float32)
    normal = (first * lax.rsqrt(lax.optimization_barrier(jnp.mean(first * first, axis=-1, keepdims=True)) + EPS) * norm_gain.astype(jnp.float32)).astype(jnp.bfloat16)
    gate_pre = jnp.dot(normal, w_gate, preferred_element_type=jnp.float32).astype(jnp.bfloat16)
    up_pre = jnp.dot(normal, w_up, preferred_element_type=jnp.float32).astype(jnp.bfloat16)
    both = jnp.concatenate([gate_pre, up_pre], axis=1).astype(jnp.float32)
    taps = jnp.concatenate([conv_gate, conv_up], axis=1).astype(jnp.float32)
    total = both.shape[0]
    padded = jnp.concatenate([jnp.zeros((2, both.shape[1]), jnp.float32), both], axis=0)
    conv = taps[0] * padded[0:total] + taps[1] * padded[1:total + 1] + taps[2] * padded[2:total + 2]
    half = w_gate.shape[1]
    hidden = (jax.nn.silu(conv[:, :half]) * conv[:, half:]).astype(jnp.bfloat16)
    mixed = first + jnp.dot(hidden, w_down, preferred_element_type=jnp.float32)
    return mixed.astype(jnp.bfloat16)
```

```python
import functools
import math

import jax
import jax.numpy as jnp
from jax import lax
from jax.experimental import pallas as pl
from jax.experimental.pallas import tpu as pltpu
from jax.sharding import PartitionSpec as P

EPS = 1e-06
NEG = -1e30
LOG2E = math.log2(math.e)
F32 = jnp.float32
BF16 = jnp.bfloat16
MESH = pl.DeviceIdType.MESH
NT = (((1,), (1,)), ((), ()))


def nt(a, b):
    return lax.dot_general(a, b, NT, preferred_element_type=F32)


def nn(a, b):
    return jnp.dot(a, b, preferred_element_type=F32)


def eye(n):
    a = lax.broadcasted_iota(jnp.int32, (n, n), 0)
    b = lax.broadcasted_iota(jnp.int32, (n, n), 1)
    return (a == b).astype(F32).astype(BF16)


def kernel(
    zn,
    yn,
    tn,
    res_ref,
    qs_ref,
    ks_ref,
    vs_ref,
    ql_ref,
    kl_ref,
    vl_ref,
    gates_ref,
    wos_ref,
    wol_ref,
    gain_ref,
    wg_ref,
    wu_ref,
    cg_ref,
    cu_ref,
    wd_ref,
    out_ref,
    gat,
    kv,
    qin,
    wa,
    wb,
    cums,
    bias,
    kk,
    acc,
    stat,
    oout,
    oin,
    sout,
    sin,
    fpo,
    fpi,
    dno,
    dni,
    first,
    ext,
    halo_out,
    halo_in,
    ebuf,
    hid,
    gat_s,
    gat_r,
    kv_s,
    kv_r,
    q_s,
    q_r,
    w1_s,
    w1_r,
    w2_s,
    w2_r,
    o_s,
    o_r,
    st_s,
    st_r,
    fp_s,
    fp_r,
    n_s,
    n_r,
    d_s,
    d_r,
    h_s,
    h_r,
):
    sp = lax.axis_index("sp")
    tp = lax.axis_index("tp")
    z = sp // yn
    y = sp - z * yn
    tok = ks_ref.shape[0]
    wrows = wg_ref.shape[0]
    half = wa.shape[3]
    own = res_ref.shape[0]
    d = res_ref.shape[1]
    hy, hz = yn // 2, zn // 2
    sends = []

    def yid(dy):
        return (z * yn + lax.rem(y + dy + yn, yn), tp)

    def zid(dz):
        return (lax.rem(z + dz + zn, zn) * yn + y, tp)

    def tid(dt):
        return (sp, lax.rem(tp + dt, tn))

    def rc(src, dst, ss, rs, dev):
        return pltpu.make_async_remote_copy(
            src_ref=src, dst_ref=dst, send_sem=ss, recv_sem=rs, device_id=dev, device_id_type=MESH
        )

    def send(src, dst, ss, rs, dev):
        c = rc(src, dst, ss, rs, dev)
        c.start()
        sends.append(c)

    def landed(dst, ss, rs):
        rc(dst, dst, ss, rs, yid(1)).wait_recv()

    barrier = pltpu.get_barrier_semaphore()
    for i in range(1, yn):
        pl.semaphore_signal(barrier, inc=1, device_id=yid(i), device_id_type=MESH)
    for i in range(1, zn):
        pl.semaphore_signal(barrier, inc=1, device_id=zid(i), device_id_type=MESH)
    for i in range(1, tn):
        pl.semaphore_signal(barrier, inc=1, device_id=tid(i), device_id_type=MESH)

    @pl.when(sp > 0)
    def _():
        pl.semaphore_signal(barrier, inc=1, device_id=(sp - 1, tn - 1), device_id_type=MESH)

    row = gates_ref[...]
    lane = lax.broadcasted_iota(jnp.int32, row.shape, 1)
    shift = 1
    while shift < tok:
        row = row + jnp.where(lane >= shift, pltpu.roll(row, shift, 1), 0.0)
        shift *= 2
    gat[y] = row
    kv[y, 0] = ks_ref[...]
    kv[y, 1] = kl_ref[...]
    unit = eye(tok)
    kv[y, 2] = nt(unit, vs_ref[...]).astype(BF16)
    kv[y, 3] = nt(unit, vl_ref[...]).astype(BF16)
    qin[0, 0] = qs_ref[...]
    qin[0, 1] = ql_ref[...]
    wdt = nt(eye(wrows), wd_ref[...]).astype(BF16)
    for h, w in enumerate((wa, wb)):
        cols = slice(h * half, (h + 1) * half)
        w[z, y, 0:wrows] = wg_ref[:, cols]
        w[z, y, wrows : 2 * wrows] = wu_ref[:, cols]
        w[z, y, 2 * wrows : 3 * wrows] = wdt[:, cols]

    extra = jnp.where(jnp.logical_and(tp == tn - 1, sp < zn * yn - 1), tn, 0)
    pl.semaphore_wait(barrier, yn + zn + tn - 3 + extra)

    for i in range(1, yn):
        send(gat.at[y], gat.at[y], gat_s.at[i], gat_r.at[i], yid(i))

    def kv_send(way, s, part):
        k = way * hy + s - 1
        o = lax.rem(y + (s - 1) * (1 if way else -1) + yn, yn)
        sl = kv.at[o, pl.ds(2 * part, 2)]
        send(sl, sl, kv_s.at[k, part], kv_r.at[k, part], yid(-1 if way else 1))

    def kv_wait(way, s, part):
        k = way * hy + s - 1
        o = lax.rem(y + s * (1 if way else -1) + yn, yn)
        landed(kv.at[o, pl.ds(2 * part, 2)], kv_s.at[k, part], kv_r.at[k, part])

    def w1_ref(axis, o):
        return wa.at[z, o] if axis == 0 else wb.at[o, y]

    def w1_part(ref, s, way, n):
        if s < n // 2:
            return ref
        step = ref.shape[0] // 2
        return ref.at[pl.ds(way * step, step)]

    def w1_send(axis, way, s):
        n, me = (yn, y) if axis == 0 else (zn, z)
        k = way * (n // 2) + s - 1
        o = lax.rem(me + (s - 1) * (1 if way else -1) + n, n)
        sl = w1_part(w1_ref(axis, o), s, way, n)
        to = (yid if axis == 0 else zid)(-1 if way else 1)
        send(sl, sl, w1_s.at[axis, k], w1_r.at[axis, k], to)

    def w1_wait(axis, way, s):
        n, me = (yn, y) if axis == 0 else (zn, z)
        k = way * (n // 2) + s - 1
        o = lax.rem(me + s * (1 if way else -1) + n, n)
        landed(w1_part(w1_ref(axis, o), s, way, n), w1_s.at[axis, k], w1_r.at[axis, k])

    def w2_part(axis, o, s, way, part):
        n, m = (zn, yn) if axis == 0 else (yn, zn)
        rows = pl.ds(0, 2 * wrows) if part == 0 else pl.ds(2 * wrows, wrows)
        if s < n // 2:
            span = pl.ds(0, m)
        else:
            span = pl.ds(way * (m // 2), m // 2)
        return wa.at[o, span, rows] if axis == 0 else wb.at[span, o, rows]

    def w2_send(axis, way, s, part):
        n, me = (zn, z) if axis == 0 else (yn, y)
        k = way * (n // 2) + s - 1
        o = lax.rem(me + (s - 1) * (1 if way else -1) + n, n)
        sl = w2_part(axis, o, s, way, part)
        to = (zid if axis == 0 else yid)(-1 if way else 1)
        send(sl, sl, w2_s.at[axis, k, part], w2_r.at[axis, k, part], to)

    def w2_wait(axis, way, s, part):
        n, me = (zn, z) if axis == 0 else (yn, y)
        k = way * (n // 2) + s - 1
        o = lax.rem(me + s * (1 if way else -1) + n, n)
        sl = w2_part(axis, o, s, way, part)
        landed(sl, w2_s.at[axis, k, part], w2_r.at[axis, k, part])

    def w2_step(axis, s, part):
        n = zn if axis == 0 else yn
        for way in (0, 1):
            if s > 1:
                w2_wait(axis, way, s - 1, part)
            if s <= n // 2:
                w2_send(axis, way, s, part)

    for part in (0, 1):
        for way in (0, 1):
            if hy > 1 or part == way:
                kv_send(way, 1, part)
    for i in range(1, zn):

        @pl.when(z - i >= 0)
        def _():
            rc(qin.at[0], qin.at[i], q_s.at[i], q_r.at[i], (sp - i * yn, tp)).start()

    for way in (0, 1):
        w1_send(1, way, 1)
        w1_send(0, way, 1)

    for i in range(1, yn):
        landed(gat.at[lax.rem(y - i + yn, yn)], gat_s.at[i], gat_r.at[i])
    before = jnp.zeros((8, tok), F32)
    for i in range(yn):
        block = gat[i]
        cums[i] = (before + block) * LOG2E
        before = before + jnp.broadcast_to(block[:, tok - 1 : tok], block.shape)
    total = before * LOG2E
    for i in range(1, zn):

        @pl.when(z + i < zn)
        def _():
            landed(qin.at[i], q_s.at[i], q_r.at[i])

    scales = (64 ** (-0.5) * LOG2E, 64 ** (-0.5) * LOG2E, 128 ** (-0.5) * LOG2E)
    spans = ((0, 64), (64, 128), (128, 256))

    def attend(o, mode):
        key_lane = lax.broadcasted_iota(jnp.int32, (tok, 128), 1)
        ksm = kv[o, 0]
        zero = jnp.zeros_like(ksm)
        kk[0:tok] = jnp.where(key_lane < 64, ksm, zero)
        kk[tok : 2 * tok] = jnp.where(key_lane < 64, zero, ksm)
        cum = cums[o]
        for h in range(3):
            bias[h] = -jnp.broadcast_to(cum[h : h + 1, :], (tok, tok)).T

        def one(i, masked):
            qsm = qin[i, 0]
            qla = qin[i, 1]
            raw = nt(kk[...], qsm)
            rawl = nt(kv[o, 1], qla)
            for h in range(3):
                s = raw[h * tok : (h + 1) * tok] if h < 2 else rawl
                s = s * scales[h] + bias[h]
                if masked:
                    a = lax.broadcasted_iota(jnp.int32, s.shape, 0)
                    b = lax.broadcasted_iota(jnp.int32, s.shape, 1)
                    s = jnp.where(a <= b, s, NEG)
                top = jnp.max(s, axis=0, keepdims=True)
                if mode > 0:
                    old = stat[i, h : h + 1]
                    top = jnp.maximum(old, top)
                    fade = jnp.exp2(old - top)
                p = jnp.exp2(s - top)
                den = jnp.sum(p, axis=0, keepdims=True)
                lo, hi = spans[h]
                vt = kv[o, 2, lo:hi] if h < 2 else kv[o, 3]
                part = nn(vt, p.astype(BF16))
                if mode > 0:
                    den = den + fade * stat[i, 3 + h : 4 + h]
                    part = part + fade * acc[i, lo:hi]
                stat[i, h : h + 1] = top
                stat[i, 3 + h : 4 + h] = den
                acc[i, lo:hi] = part

        def step(i, c):
            one(i, False)
            if mode == 2:

                @pl.when(i > 0)
                def _():
                    oout[i] = acc[i].astype(BF16)
                    sout[i, 0:8] = stat[i]
                    sout[i, 8:16] = total
                    to = (sp + i * yn, tp)
                    rc(oout.at[i], oin.at[i], o_s.at[i], o_r.at[i], to).start()
                    rc(sout.at[i], sin.at[i], st_s.at[i], st_r.at[i], to).start()

            return c

        if mode == 0:
            one(0, True)
            lax.fori_loop(1, zn - z, step, 0)
        else:
            lax.fori_loop(jnp.where(o < y, 0, 1), zn - z, step, 0)

    attend(y, 0)
    for s in range(1, hy + 1):
        for part in (0, 1):
            for way in (0, 1):
                if s < hy or part == way:
                    kv_wait(way, s, part)
                if s + 1 < hy or (s + 1 == hy and part == way):
                    kv_send(way, s + 1, part)
        for axis, n in ((1, zn), (0, yn)):
            for way in (0, 1):
                if s <= n // 2:
                    w1_wait(axis, way, s)
                if s + 1 <= n // 2:
                    w1_send(axis, way, s + 1)
        if s == hy:
            for axis in (0, 1):
                for part in (0, 1):
                    w2_step(axis, 1, part)
            attend(lax.rem(y + hy, yn), 2)
        else:
            attend(lax.rem(y - s + yn, yn), 1)
            attend(lax.rem(y + s, yn), 1)

    def merge(i, gap):
        landed(oin.at[i], o_s.at[i], o_r.at[i])
        landed(sin.at[i], st_s.at[i], st_r.at[i])
        gap = gap + sin[i, 8:16]
        for h in range(3):
            lo, hi = spans[h]
            old = stat[0, h : h + 1]
            new = sin[i, h : h + 1] + gap[h : h + 1]
            top = jnp.maximum(old, new)
            a = jnp.exp2(old - top)
            b = jnp.exp2(new - top)
            stat[0, h : h + 1] = top
            stat[0, 3 + h : 4 + h] = a * stat[0, 3 + h : 4 + h] + b * sin[i, 3 + h : 4 + h]
            acc[0, lo:hi] = a * acc[0, lo:hi] + b * oin[i, lo:hi].astype(F32)
        return gap

    lax.fori_loop(1, z + 1, merge, jnp.zeros((8, tok), F32))
    normed = []
    for h in range(3):
        lo, hi = spans[h]
        att = acc[0, lo:hi] / stat[0, 3 + h : 4 + h]
        mean = jnp.mean(att * att, axis=0, keepdims=True)
        normed.append(att * lax.rsqrt(mean + EPS))
    nsm = jnp.concatenate(normed[:2], axis=0).T.astype(BF16)
    nla = normed[2].T.astype(BF16)
    width = min(512, d)
    for c in range(d // width):
        cols = slice(c * width, (c + 1) * width)
        fpo[:, cols] = (nn(nsm, wos_ref[:, cols]) + nn(nla, wol_ref[:, cols])).astype(BF16)

    def mine(ref, t):
        return ref.at[pl.ds(pl.multiple_of(t * own, own), own)]

    for i in range(1, tn):
        send(mine(fpo, lax.rem(tp + i, tn)), fpi.at[i], fp_s.at[i], fp_r.at[i], tid(i))
    for axis in (0, 1):
        for part in (0, 1):
            w2_step(axis, 2, part)
    value = res_ref[...].astype(F32) + mine(fpo, tp)[...].astype(F32)
    for i in range(1, tn):
        landed(fpi.at[i], fp_s.at[i], fp_r.at[i])
        value = value + fpi[i].astype(F32)
    first[...] = value
    mean = jnp.mean(value * value, axis=1, keepdims=True)
    normal = value * lax.rsqrt(mean + EPS) * gain_ref[...]
    ext[0:16] = jnp.zeros((16, d), BF16)
    place = ext.at[pl.ds(pl.multiple_of(16 + tp * own, 16), own)]
    place[...] = normal.astype(BF16)
    for i in range(1, tn):
        send(place, place, n_s.at[i], n_r.at[i], tid(i))
    hw = d // 8

    @pl.when(jnp.logical_and(tp == tn - 1, sp < zn * yn - 1))
    def _():
        rows = [normal[own - 2 : own, c * hw : (c + 1) * hw] for c in range(8)]
        halo_out[...] = jnp.concatenate(rows, axis=0).astype(BF16)
        for i in range(tn):
            rc(halo_out, halo_in, h_s.at[i], h_r, (sp + 1, i)).start()

    for axis in (0, 1):
        for part in (0, 1):
            w2_step(axis, 3, part)

    @pl.when(sp > 0)
    def _():
        landed(halo_in, h_s.at[0], h_r)
        block = halo_in[...].astype(F32)
        for c in range(8):
            pad = jnp.zeros((14, hw), F32)
            rim = jnp.concatenate([pad, block[2 * c : 2 * c + 2]], axis=0)
            ext[0:16, c * hw : (c + 1) * hw] = rim.astype(BF16)

    for i in range(1, tn):
        src = lax.rem(tp - i + tn, tn)
        landed(ext.at[pl.ds(pl.multiple_of(16 + src * own, 16), own)], n_s.at[i], n_r.at[i])
    for axis in (0, 1):
        for part in (0, 1):
            w2_step(axis, 4, part)
    for s in (hz + 1,):
        w2_step(0, s, 0)
    for s in (hy + 1,):
        w2_step(1, s, 0)

    count = zn * yn
    for h, (w, _n) in enumerate(((wa, 0), (wb, 1))):
        cols = slice(h * half, (h + 1) * half)
        conv = []
        for j, taps in ((0, cg_ref), (1, cu_ref)):
            weight = w[:, :, j * wrows : (j + 1) * wrows].reshape(count * wrows, half)
            ebuf[j] = nn(ext[...], weight).astype(BF16).astype(F32)
            conv.append(
                taps[0:1, cols] * ebuf[j, 14 : 14 + tok]
                + taps[1:2, cols] * ebuf[j, 15 : 15 + tok]
                + taps[2:3, cols] * ebuf[j, 16 : 16 + tok]
            )
        hid[h] = (conv[0] / (1.0 + jnp.exp(-conv[0])) * conv[1]).astype(BF16)

    w2_step(0, hz + 1, 1)
    w2_step(1, hy + 1, 1)
    zs = max(1, zn // 4)
    for c in range(zn // zs):
        span = zs * yn * wrows
        total_down = None
        for h, w in enumerate((wa, wb)):
            weight = w[c * zs : (c + 1) * zs, :, 2 * wrows : 3 * wrows].reshape(span, half)
            term = nt(hid[h], weight)
            total_down = term if total_down is None else total_down + term
        dno[:, c * span : (c + 1) * span] = total_down.astype(BF16)
    for i in range(1, tn):
        send(mine(dno, lax.rem(tp + i, tn)), dni.at[i], d_s.at[i], d_r.at[i], tid(i))
    value = first[...] + mine(dno, tp)[...].astype(F32)
    for i in range(1, tn):
        landed(dni.at[i], d_s.at[i], d_r.at[i])
        value = value + dni[i].astype(F32)
    out_ref[...] = value.astype(BF16)

    for c in sends:
        c.wait_send()
    for i in range(1, zn):

        @pl.when(z - i >= 0)
        def _():
            rc(qin.at[0], qin.at[i], q_s.at[i], q_r.at[i], yid(1)).wait_send()

        @pl.when(z + i < zn)
        def _():
            rc(oout.at[i], oin.at[i], o_s.at[i], o_r.at[i], yid(1)).wait_send()
            rc(sout.at[i], sin.at[i], st_s.at[i], st_r.at[i], yid(1)).wait_send()

    @pl.when(jnp.logical_and(tp == tn - 1, sp < zn * yn - 1))
    def _():
        for i in range(tn):
            rc(halo_out, halo_in, h_s.at[i], h_r, yid(1)).wait_send()


def body(
    sizes,
    residual,
    q_small,
    k_small,
    v_small,
    q_large,
    k_large,
    v_large,
    forget_small,
    forget_large,
    w_out_small,
    w_out_large,
    norm_gain,
    w_gate,
    w_up,
    conv_gate,
    conv_up,
    w_down,
):
    zn, yn, tn = sizes
    tok = q_small.shape[0]
    own, d = residual.shape
    wrows, ff = w_gate.shape
    half = ff // 2
    gates = jnp.concatenate([forget_small, forget_large], axis=1)
    gates = jnp.pad(jax.nn.log_sigmoid(gates).T, ((0, 5), (0, 0)))
    dma = pltpu.SemaphoreType.DMA
    hy, hz = yn // 2, zn // 2
    scratch = [
        pltpu.VMEM((yn, 8, tok), F32),
        pltpu.VMEM((yn, 4, tok, 128), BF16),
        pltpu.VMEM((zn, 2, tok, 128), BF16),
        pltpu.VMEM((zn, yn, 3 * wrows, half), BF16),
        pltpu.VMEM((zn, yn, 3 * wrows, half), BF16),
        pltpu.VMEM((yn, 8, tok), F32),
        pltpu.VMEM((3, tok, tok), F32),
        pltpu.VMEM((2 * tok, 128), BF16),
        pltpu.VMEM((zn, 256, tok), F32),
        pltpu.VMEM((zn, 8, tok), F32),
        pltpu.VMEM((zn, 256, tok), BF16),
        pltpu.VMEM((zn, 256, tok), BF16),
        pltpu.VMEM((zn, 16, tok), F32),
        pltpu.VMEM((zn, 16, tok), F32),
        pltpu.VMEM((tok, d), BF16),
        pltpu.VMEM((tn, own, d), BF16),
        pltpu.VMEM((tok, d), BF16),
        pltpu.VMEM((tn, own, d), BF16),
        pltpu.VMEM((own, d), F32),
        pltpu.VMEM((tok + 16, d), BF16),
        pltpu.VMEM((16, d // 8), BF16),
        pltpu.VMEM((16, d // 8), BF16),
        pltpu.VMEM((2, tok + 16, half), F32),
        pltpu.VMEM((2, tok, half), BF16),
        dma((yn,)),
        dma((yn,)),
        dma((yn, 2)),
        dma((yn, 2)),
        dma((zn,)),
        dma((zn,)),
        dma((2, max(yn, zn))),
        dma((2, max(yn, zn))),
        dma((2, max(yn, zn), 2)),
        dma((2, max(yn, zn), 2)),
        dma((zn,)),
        dma((zn,)),
        dma((zn,)),
        dma((zn,)),
        dma((tn,)),
        dma((tn,)),
        dma((tn,)),
        dma((tn,)),
        dma((tn,)),
        dma((tn,)),
        dma((tn,)),
        dma,
    ]
    return pl.pallas_call(
        functools.partial(kernel, zn, yn, tn),
        out_shape=jax.ShapeDtypeStruct((own, d), BF16),
        in_specs=[pl.BlockSpec(memory_space=pltpu.VMEM)] * 16,
        out_specs=pl.BlockSpec(memory_space=pltpu.VMEM),
        scratch_shapes=scratch,
        compiler_params=pltpu.CompilerParams(
            collective_id=0, has_side_effects=True, vmem_limit_bytes=60 * 1024 * 1024
        ),
    )(
        residual,
        q_small,
        k_small,
        v_small,
        q_large,
        k_large,
        v_large,
        gates,
        w_out_small,
        w_out_large,
        norm_gain.reshape(1, d),
        w_gate,
        w_up,
        conv_gate,
        conv_up,
        w_down,
    )


def solution(mesh):
    sp = mesh.shape["sp"]
    yn = math.isqrt(sp)
    zn = sp // yn
    placed = (
        P(("sp", "tp"), None),
        P("sp", "tp"),
        P("sp", "tp"),
        P("sp", "tp"),
        P("sp", "tp"),
        P("sp", "tp"),
        P("sp", "tp"),
        P("sp", "tp"),
        P("sp", "tp"),
        P("tp", None),
        P("tp", None),
        P(),
        P("sp", "tp"),
        P("sp", "tp"),
        P(None, "tp"),
        P(None, "tp"),
        P("tp", "sp"),
    )
    return jax.shard_map(
        functools.partial(body, (zn, yn, mesh.shape["tp"])),
        mesh=mesh,
        in_specs=placed,
        out_specs=P(("sp", "tp"), None),
        check_vma=False,
    )
```

```python
import functools
import math

import jax
import jax.numpy as jnp
from jax import lax
from jax.experimental import pallas as pl
from jax.experimental.pallas import tpu as pltpu
from jax.sharding import PartitionSpec as P

EPS = 1e-06
NEG = -1e30
LOG2E = math.log2(math.e)
F32 = jnp.float32
BF16 = jnp.bfloat16
MESH = pl.DeviceIdType.MESH
NT = (((1,), (1,)), ((), ()))


def nt(a, b):
    return lax.dot_general(a, b, NT, preferred_element_type=F32)


def nn(a, b):
    return jnp.dot(a, b, preferred_element_type=F32)


def eye(n):
    a = lax.broadcasted_iota(jnp.int32, (n, n), 0)
    b = lax.broadcasted_iota(jnp.int32, (n, n), 1)
    return (a == b).astype(F32).astype(BF16)


def kernel(
    zn,
    yn,
    tn,
    res_ref,
    qs_ref,
    ks_ref,
    vs_ref,
    ql_ref,
    kl_ref,
    vl_ref,
    fs_ref,
    fl_ref,
    wos_hbm,
    wol_hbm,
    gain_ref,
    wg_ref,
    wu_ref,
    cg_ref,
    cu_ref,
    wd_ref,
    out_ref,
    wos_ref,
    wol_ref,
    gat,
    gatz,
    ty,
    tz,
    wa,
    wb,
    cums,
    biass,
    biasl,
    edge,
    kks,
    kkl,
    vvs,
    vvl,
    accs,
    accl,
    stats,
    statl,
    oout,
    oin,
    sout,
    sin,
    fpo,
    fpi,
    dno,
    dni,
    first,
    ext,
    halo_out,
    halo_in,
    ebuf,
    hid,
    loc_s,
    gat_s,
    gat_r,
    t_s,
    t_r,
    w1_s,
    w1_r,
    w2_s,
    w2_r,
    o_s,
    o_r,
    st_s,
    st_r,
    fp_s,
    fp_r,
    n_s,
    n_r,
    d_s,
    d_r,
    h_s,
    h_r,
):
    sp = lax.axis_index("sp")
    tp = lax.axis_index("tp")
    z = sp // yn
    y = sp - z * yn
    tok = ks_ref.shape[0]
    wrows = wg_ref.shape[0]
    half = wa.shape[3]
    own = res_ref.shape[0]
    d = res_ref.shape[1]
    hy, hz = yn // 2, zn // 2
    sends = []

    def yid(dy):
        return (z * yn + lax.rem(y + dy + yn, yn), tp)

    def zid(dz):
        return (lax.rem(z + dz + zn, zn) * yn + y, tp)

    def tid(dt):
        return (sp, lax.rem(tp + dt, tn))

    def rc(src, dst, ss, rs, dev):
        return pltpu.make_async_remote_copy(
            src_ref=src, dst_ref=dst, send_sem=ss, recv_sem=rs, device_id=dev, device_id_type=MESH
        )

    def send(src, dst, ss, rs, dev):
        c = rc(src, dst, ss, rs, dev)
        c.start()
        sends.append(c)

    def landed(dst, ss, rs):
        rc(dst, dst, ss, rs, yid(1)).wait_recv()

    barrier = pltpu.get_barrier_semaphore()
    for i in range(1, yn):
        pl.semaphore_signal(barrier, inc=1, device_id=yid(i), device_id_type=MESH)
    for i in range(1, zn):
        pl.semaphore_signal(barrier, inc=1, device_id=zid(i), device_id_type=MESH)
    for i in range(1, tn):
        pl.semaphore_signal(barrier, inc=1, device_id=tid(i), device_id_type=MESH)

    @pl.when(sp > 0)
    def _():
        pl.semaphore_signal(barrier, inc=1, device_id=(sp - 1, tn - 1), device_id_type=MESH)

    loads = [
        pltpu.make_async_copy(wos_hbm, wos_ref, loc_s.at[0]),
        pltpu.make_async_copy(wol_hbm, wol_ref, loc_s.at[1]),
    ]
    for c in loads:
        c.start()

    def log_gate(x):
        u = jnp.exp(-jnp.abs(x))
        series = u * (1.0 - u * (0.5 - u * (1.0 / 3.0 - u * 0.25)))
        return jnp.minimum(x, 0.0) - jnp.where(u < 0.01, series, jnp.log(1.0 + u))

    row = jnp.concatenate(
        [log_gate(fs_ref[...]), log_gate(fl_ref[...]), jnp.zeros((5, tok), F32)], axis=0
    )
    lane = lax.broadcasted_iota(jnp.int32, row.shape, 1)
    shift = 1
    while shift < tok:
        row = row + jnp.where(lane >= shift, pltpu.roll(row, shift, 1), 0.0)
        shift *= 2
    gat[y] = row
    unit = eye(tok)
    ty[y, 0] = ks_ref[...]
    ty[y, 1] = nt(unit, vs_ref[...]).astype(BF16)
    ty[y, 2] = ql_ref[...]
    tz[z, 0] = kl_ref[...]
    tz[z, 1] = nt(unit, vl_ref[...]).astype(BF16)
    tz[z, 2] = qs_ref[...]
    for h, w in enumerate((wa, wb)):
        cols = slice(h * half, (h + 1) * half)
        w[z, y, 0:wrows] = wg_ref[:, cols]
        w[z, y, wrows : 2 * wrows] = wu_ref[:, cols]
        w[z, y, 2 * wrows : 3 * wrows] = wd_ref[:, cols]
    ext[0:16] = jnp.zeros((16, d), BF16)

    extra = jnp.where(jnp.logical_and(tp == tn - 1, sp < zn * yn - 1), tn, 0)
    pl.semaphore_wait(barrier, yn + zn + tn - 3 + extra)

    for i in range(1, yn):
        send(gat.at[y], gat.at[y], gat_s.at[0, i], gat_r.at[0, i], yid(i))

    def part_of(ref, s, way, n, dim):
        if s < n // 2:
            return ref
        step = ref.shape[dim] // 2
        cut = pl.ds(way * step, step)
        return ref.at[cut] if dim == 0 else ref.at[:, cut]

    def ring(axis, way, s, kind, start):
        n, me = (yn, y) if axis == 0 else (zn, z)
        k = way * (n // 2) + s - 1
        hop = s - 1 if start else s
        o = lax.rem(me + hop * (1 if way else -1) + n, n)
        if kind == 0:
            ref = part_of((ty if axis == 0 else tz).at[o], s, way, n, 1)
            ss, rs = t_s.at[axis, k], t_r.at[axis, k]
        else:
            ref = part_of(wa.at[z, o] if axis == 0 else wb.at[o, y], s, way, n, 0)
            ss, rs = w1_s.at[axis, k], w1_r.at[axis, k]
        if start:
            send(ref, ref, ss, rs, (yid if axis == 0 else zid)(-1 if way else 1))
        else:
            landed(ref, ss, rs)

    def w2_part(axis, o, s, way, part):
        n, m = (zn, yn) if axis == 0 else (yn, zn)
        rows = pl.ds(0, 2 * wrows) if part == 0 else pl.ds(2 * wrows, wrows)
        if s < n // 2:
            span = pl.ds(0, m)
        else:
            span = pl.ds(way * (m // 2), m // 2)
        return wa.at[o, span, rows] if axis == 0 else wb.at[span, o, rows]

    def w2_send(axis, way, s, part):
        n, me = (zn, z) if axis == 0 else (yn, y)
        k = way * (n // 2) + s - 1
        o = lax.rem(me + (s - 1) * (1 if way else -1) + n, n)
        sl = w2_part(axis, o, s, way, part)
        to = (zid if axis == 0 else yid)(-1 if way else 1)
        send(sl, sl, w2_s.at[axis, k, part], w2_r.at[axis, k, part], to)

    def w2_wait(axis, way, s, part):
        n, me = (zn, z) if axis == 0 else (yn, y)
        k = way * (n // 2) + s - 1
        o = lax.rem(me + s * (1 if way else -1) + n, n)
        sl = w2_part(axis, o, s, way, part)
        landed(sl, w2_s.at[axis, k, part], w2_r.at[axis, k, part])

    def w2_step(s, part):
        for axis, n in ((0, zn), (1, yn)):
            for way in (0, 1):
                if 1 < s <= n // 2 + 1:
                    w2_wait(axis, way, s - 1, part)
                if s <= n // 2:
                    w2_send(axis, way, s, part)

    for kind in (0, 1):
        for axis in (0, 1):
            for way in (0, 1):
                ring(axis, way, 1, kind, True)

    for i in range(1, yn):
        landed(gat.at[lax.rem(y - i + yn, yn)], gat_s.at[0, i], gat_r.at[0, i])
    before = jnp.zeros((8, tok), F32)
    for i in range(yn):
        block = gat[i]
        cums[i] = (before + block) * LOG2E
        before = before + jnp.broadcast_to(block[:, tok - 1 : tok], block.shape)
    gatz[z, 0:8] = cums[y]
    gatz[z, 8:16] = before * LOG2E
    for i in range(1, zn):
        send(gatz.at[z], gatz.at[z], gat_s.at[1, i], gat_r.at[1, i], zid(i))
    for i in range(yn):
        for h in range(2):
            column = -jnp.broadcast_to(cums[i, h : h + 1, :], (tok, tok)).T
            biass[h, i * tok : (i + 1) * tok] = column

    for s in range(1, max(hy, hz) + 1):
        for kind in (0, 1):
            for axis, n in ((0, yn), (1, zn)):
                for way in (0, 1):
                    if s <= n // 2:
                        ring(axis, way, s, kind, False)
                    if s + 1 <= n // 2:
                        ring(axis, way, s + 1, kind, True)
        if s == 1:
            for i in range(1, zn):
                landed(gatz.at[lax.rem(z - i + zn, zn)], gat_s.at[1, i], gat_r.at[1, i])
            gap = jnp.zeros((8, tok), F32)
            for i in reversed(range(zn)):
                gap = jnp.where(i < z, gap + gatz[i, 8:16], 0.0)
                away = jnp.where(i > z, -NEG, gatz[i, 2:3] - gap[2:3])
                column = -jnp.broadcast_to(away, (tok, tok)).T
                biasl[i * tok : (i + 1) * tok] = column
            edge[...] = -jnp.broadcast_to(gatz[z, 2:3], (tok, tok)).T

    w2_step(1, 0)
    key_lane = lax.broadcasted_iota(jnp.int32, (tok, 128), 1)
    for i in range(yn):
        rows = slice(i * tok, (i + 1) * tok)
        ksm = ty[i, 0]
        zero = jnp.zeros_like(ksm)
        kks[0, rows] = jnp.where(key_lane < 64, ksm, zero)
        kks[1, rows] = jnp.where(key_lane < 64, zero, ksm)
        vvs[:, rows] = ty[i, 1]
    for i in range(zn):
        rows = slice(i * tok, (i + 1) * tok)
        kkl[rows] = tz[i, 0]
        vvl[:, rows] = tz[i, 1]

    def soft(keys, query, shift, scale, values, keep):
        s = nt(keys, query) * scale + shift
        if keep is not None:
            s = jnp.where(keep, s, NEG)
        top = jnp.max(s, axis=0, keepdims=True)
        p = jnp.exp2(s - top)
        den = jnp.sum(p, axis=0, keepdims=True)
        return top, den, nn(values, p.astype(BF16))

    def small(i, keep):
        query = tz[z + i, 2]
        for h in range(2):
            lo, hi = 64 * h, 64 * h + 64
            top, den, part = soft(
                kks[h], query, biass[h], 64 ** (-0.5) * LOG2E, vvs[lo:hi], keep
            )
            stats[i, h : h + 1] = top
            stats[i, 2 + h : 3 + h] = den
            accs[i, lo:hi] = part

    def small_step(i, c):
        small(i, None)
        oout[0, i] = accs[i].astype(BF16)
        sout[0, i] = stats[i]
        to = (sp + i * yn, tp)
        rc(oout.at[0, i], oin.at[0, i], o_s.at[0, i], o_r.at[0, i], to).start()
        rc(sout.at[0, i], sin.at[0, i], st_s.at[0, i], st_r.at[0, i], to).start()
        return c

    lax.fori_loop(1, zn - z, small_step, 0)

    def large(i, c):
        o = lax.rem(y + i, yn)
        a = lax.broadcasted_iota(jnp.int32, (tok, tok), 0)
        b = lax.broadcasted_iota(jnp.int32, (tok, tok), 1)
        rows = pl.ds(pl.multiple_of(z * tok, tok), tok)
        biasl[rows] = jnp.where(y * tok + a <= o * tok + b, edge[...], NEG)
        top, den, part = soft(
            kkl[...], ty[o, 2], biasl[...], 128 ** (-0.5) * LOG2E, vvl[...], None
        )
        statl[i, 0:1] = top
        statl[i, 2:3] = den
        accl[i] = part

        @pl.when(jnp.logical_and(i > 0, jnp.logical_or(z > 0, o > y)))
        def _():
            oout[1, i] = part.astype(BF16)
            sout[1, i] = statl[i]
            to = (z * yn + o, tp)
            rc(oout.at[1, i], oin.at[1, i], o_s.at[1, i], o_r.at[1, i], to).start()
            rc(sout.at[1, i], sin.at[1, i], st_s.at[1, i], st_r.at[1, i], to).start()

        return c

    lax.fori_loop(0, yn, large, 0)
    a = lax.broadcasted_iota(jnp.int32, (yn * tok, tok), 0)
    b = lax.broadcasted_iota(jnp.int32, (yn * tok, tok), 1)
    small(0, a <= y * tok + b)
    w2_step(1, 1)
    w2_step(2, 0)

    def fold(acc, stat, slot, lo, hi, i, row, gap):
        old = stat[0, row : row + 1]
        new = sin[slot, i, row : row + 1]
        if gap is not None:
            new = new + gap
        top = jnp.maximum(old, new)
        a = jnp.exp2(old - top)
        b = jnp.exp2(new - top)
        stat[0, row : row + 1] = top
        den = a * stat[0, 2 + row : 3 + row] + b * sin[slot, i, 2 + row : 3 + row]
        stat[0, 2 + row : 3 + row] = den
        acc[0, lo:hi] = a * acc[0, lo:hi] + b * oin[slot, i, lo:hi].astype(F32)

    def merge(i, gap):
        landed(oin.at[0, i], o_s.at[0, i], o_r.at[0, i])
        landed(sin.at[0, i], st_s.at[0, i], st_r.at[0, i])
        gap = gap + gatz[z - i, 8:16]
        for h in range(2):
            fold(accs, stats, 0, 64 * h, 64 * h + 64, i, h, gap[h : h + 1])
        return gap

    lax.fori_loop(1, z + 1, merge, jnp.zeros((8, tok), F32))

    def merge_large(i, c):
        @pl.when(jnp.logical_or(z > 0, lax.rem(y - i + yn, yn) < y))
        def _():
            landed(oin.at[1, i], o_s.at[1, i], o_r.at[1, i])
            landed(sin.at[1, i], st_s.at[1, i], st_r.at[1, i])
            fold(accl, statl, 1, 0, 128, i, 0, None)

        return c

    lax.fori_loop(1, yn, merge_large, 0)
    normed = []
    for h in range(3):
        if h < 2:
            att = accs[0, 64 * h : 64 * h + 64] / stats[0, 2 + h : 3 + h]
        else:
            att = accl[0] / statl[0, 2:3]
        mean = jnp.mean(att * att, axis=0, keepdims=True)
        normed.append(att * lax.rsqrt(mean + EPS))
    nsm = jnp.concatenate(normed[:2], axis=0).T.astype(BF16)
    nla = normed[2].T.astype(BF16)
    for c in loads:
        c.wait()
    width = min(512, d)
    for c in range(d // width):
        cols = slice(c * width, (c + 1) * width)
        fpo[:, cols] = (nn(nsm, wos_ref[:, cols]) + nn(nla, wol_ref[:, cols])).astype(BF16)

    def mine(ref, t):
        return ref.at[pl.ds(pl.multiple_of(t * own, own), own)]

    for i in range(1, tn):
        send(mine(fpo, lax.rem(tp + i, tn)), fpi.at[i], fp_s.at[i], fp_r.at[i], tid(i))
    w2_step(2, 1)
    value = res_ref[...].astype(F32) + mine(fpo, tp)[...].astype(F32)
    for i in range(1, tn):
        landed(fpi.at[i], fp_s.at[i], fp_r.at[i])
        value = value + fpi[i].astype(F32)
    first[...] = value
    mean = jnp.mean(value * value, axis=1, keepdims=True)
    normal = value * lax.rsqrt(mean + EPS) * gain_ref[...]
    place = ext.at[pl.ds(pl.multiple_of(16 + tp * own, 16), own)]
    place[...] = normal.astype(BF16)
    for i in range(1, tn):
        send(place, place, n_s.at[i], n_r.at[i], tid(i))
    hw = d // 8

    @pl.when(jnp.logical_and(tp == tn - 1, sp < zn * yn - 1))
    def _():
        rows = [normal[own - 2 : own, c * hw : (c + 1) * hw] for c in range(8)]
        halo_out[...] = jnp.concatenate(rows, axis=0).astype(BF16)
        for i in range(tn):
            rc(halo_out, halo_in, h_s.at[i], h_r, (sp + 1, i)).start()

    w2_step(3, 0)
    w2_step(3, 1)

    @pl.when(sp > 0)
    def _():
        landed(halo_in, h_s.at[0], h_r)
        block = halo_in[...].astype(F32)
        for c in range(8):
            pad = jnp.zeros((14, hw), F32)
            rim = jnp.concatenate([pad, block[2 * c : 2 * c + 2]], axis=0)
            ext[0:16, c * hw : (c + 1) * hw] = rim.astype(BF16)

    for i in range(1, tn):
        src = lax.rem(tp - i + tn, tn)
        landed(ext.at[pl.ds(pl.multiple_of(16 + src * own, 16), own)], n_s.at[i], n_r.at[i])
    w2_step(4, 0)
    w2_step(4, 1)
    w2_step(5, 0)

    count = zn * yn
    for h, (w, _n) in enumerate(((wa, 0), (wb, 1))):
        cols = slice(h * half, (h + 1) * half)
        conv = []
        for j, taps in ((0, cg_ref), (1, cu_ref)):
            weight = w[:, :, j * wrows : (j + 1) * wrows].reshape(count * wrows, half)
            ebuf[j] = nn(ext[...], weight).astype(BF16).astype(F32)
            conv.append(
                taps[0:1, cols] * ebuf[j, 14 : 14 + tok]
                + taps[1:2, cols] * ebuf[j, 15 : 15 + tok]
                + taps[2:3, cols] * ebuf[j, 16 : 16 + tok]
            )
        hid[h] = (conv[0] / (1.0 + jnp.exp(-conv[0])) * conv[1]).astype(BF16)

    w2_step(5, 1)
    zs = max(1, zn // 4)
    for c in range(zn // zs):
        span = zs * yn * wrows
        total_down = None
        for h, w in enumerate((wa, wb)):
            weight = w[c * zs : (c + 1) * zs, :, 2 * wrows : 3 * wrows].reshape(span, half)
            term = nt(hid[h], weight)
            total_down = term if total_down is None else total_down + term
        dno[:, c * span : (c + 1) * span] = total_down.astype(BF16)
    for i in range(1, tn):
        send(mine(dno, lax.rem(tp + i, tn)), dni.at[i], d_s.at[i], d_r.at[i], tid(i))
    value = first[...] + mine(dno, tp)[...].astype(F32)
    for i in range(1, tn):
        landed(dni.at[i], d_s.at[i], d_r.at[i])
        value = value + dni[i].astype(F32)
    out_ref[...] = value.astype(BF16)

    for c in sends:
        c.wait_send()
    for i in range(1, zn):

        @pl.when(z + i < zn)
        def _():
            rc(oout.at[0, i], oin.at[0, i], o_s.at[0, i], o_r.at[0, i], yid(1)).wait_send()
            rc(sout.at[0, i], sin.at[0, i], st_s.at[0, i], st_r.at[0, i], yid(1)).wait_send()

    for i in range(1, yn):

        @pl.when(jnp.logical_or(z > 0, lax.rem(y + i, yn) > y))
        def _():
            rc(oout.at[1, i], oin.at[1, i], o_s.at[1, i], o_r.at[1, i], yid(1)).wait_send()
            rc(sout.at[1, i], sin.at[1, i], st_s.at[1, i], st_r.at[1, i], yid(1)).wait_send()

    @pl.when(jnp.logical_and(tp == tn - 1, sp < zn * yn - 1))
    def _():
        for i in range(tn):
            rc(halo_out, halo_in, h_s.at[i], h_r, yid(1)).wait_send()


def body(
    sizes,
    residual,
    q_small,
    k_small,
    v_small,
    q_large,
    k_large,
    v_large,
    forget_small,
    forget_large,
    w_out_small,
    w_out_large,
    norm_gain,
    w_gate,
    w_up,
    conv_gate,
    conv_up,
    w_down,
):
    zn, yn, tn = sizes
    tok = q_small.shape[0]
    own, d = residual.shape
    wrows, ff = w_gate.shape
    half = ff // 2
    dma = pltpu.SemaphoreType.DMA
    big = max(yn, zn)
    scratch = [
        pltpu.VMEM(w_out_small.shape, BF16),
        pltpu.VMEM(w_out_large.shape, BF16),
        pltpu.VMEM((yn, 8, tok), F32),
        pltpu.VMEM((zn, 16, tok), F32),
        pltpu.VMEM((yn, 3, tok, 128), BF16),
        pltpu.VMEM((zn, 3, tok, 128), BF16),
        pltpu.VMEM((zn, yn, 3 * wrows, half), BF16),
        pltpu.VMEM((zn, yn, 3 * wrows, half), BF16),
        pltpu.VMEM((yn, 8, tok), F32),
        pltpu.VMEM((2, yn * tok, tok), F32),
        pltpu.VMEM((zn * tok, tok), F32),
        pltpu.VMEM((tok, tok), F32),
        pltpu.VMEM((2, yn * tok, 128), BF16),
        pltpu.VMEM((zn * tok, 128), BF16),
        pltpu.VMEM((128, yn * tok), BF16),
        pltpu.VMEM((128, zn * tok), BF16),
        pltpu.VMEM((zn, 128, tok), F32),
        pltpu.VMEM((yn, 128, tok), F32),
        pltpu.VMEM((zn, 8, tok), F32),
        pltpu.VMEM((yn, 8, tok), F32),
        pltpu.VMEM((2, big, 128, tok), BF16),
        pltpu.VMEM((2, big, 128, tok), BF16),
        pltpu.VMEM((2, big, 8, tok), F32),
        pltpu.VMEM((2, big, 8, tok), F32),
        pltpu.VMEM((tok, d), BF16),
        pltpu.VMEM((tn, own, d), BF16),
        pltpu.VMEM((tok, d), BF16),
        pltpu.VMEM((tn, own, d), BF16),
        pltpu.VMEM((own, d), F32),
        pltpu.VMEM((tok + 16, d), BF16),
        pltpu.VMEM((16, d // 8), BF16),
        pltpu.VMEM((16, d // 8), BF16),
        pltpu.VMEM((2, tok + 16, half), F32),
        pltpu.VMEM((2, tok, half), BF16),
        dma((2,)),
        dma((2, big)),
        dma((2, big)),
        dma((2, big)),
        dma((2, big)),
        dma((2, big)),
        dma((2, big)),
        dma((2, big, 2)),
        dma((2, big, 2)),
        dma((2, big)),
        dma((2, big)),
        dma((2, big)),
        dma((2, big)),
        dma((tn,)),
        dma((tn,)),
        dma((tn,)),
        dma((tn,)),
        dma((tn,)),
        dma((tn,)),
        dma((tn,)),
        dma,
    ]
    vmem = pl.BlockSpec(memory_space=pltpu.VMEM)
    hbm = pl.BlockSpec(memory_space=pl.ANY)
    return pl.pallas_call(
        functools.partial(kernel, zn, yn, tn),
        out_shape=jax.ShapeDtypeStruct((own, d), BF16),
        in_specs=[vmem] * 9 + [hbm] * 2 + [vmem] * 6,
        out_specs=pl.BlockSpec(memory_space=pltpu.VMEM),
        scratch_shapes=scratch,
        compiler_params=pltpu.CompilerParams(
            collective_id=0, has_side_effects=True, vmem_limit_bytes=60 * 1024 * 1024
        ),
    )(
        residual,
        q_small,
        k_small,
        v_small,
        q_large,
        k_large,
        v_large,
        forget_small.T,
        forget_large.T,
        w_out_small,
        w_out_large,
        norm_gain.reshape(1, d),
        w_gate,
        w_up,
        conv_gate,
        conv_up,
        w_down.T,
    )


def solution(mesh):
    sp = mesh.shape["sp"]
    yn = math.isqrt(sp)
    zn = sp // yn
    placed = (
        P(("sp", "tp"), None),
        P("sp", "tp"),
        P("sp", "tp"),
        P("sp", "tp"),
        P("sp", "tp"),
        P("sp", "tp"),
        P("sp", "tp"),
        P("sp", "tp"),
        P("sp", "tp"),
        P("tp", None),
        P("tp", None),
        P(),
        P("sp", "tp"),
        P("sp", "tp"),
        P(None, "tp"),
        P(None, "tp"),
        P("tp", "sp"),
    )
    return jax.shard_map(
        functools.partial(body, (zn, yn, mesh.shape["tp"])),
        mesh=mesh,
        in_specs=placed,
        out_specs=P(("sp", "tp"), None),
        check_vma=False,
    )
```

```python
import functools
import math

import jax
import jax.numpy as jnp
from jax import lax
from jax.experimental import pallas as pl
from jax.experimental.pallas import tpu as pltpu
from jax.sharding import PartitionSpec as P

EPS = 1e-06
NEG = -1e30
LOG2E = math.log2(math.e)
F32 = jnp.float32
BF16 = jnp.bfloat16
MESH = pl.DeviceIdType.MESH
NT = (((1,), (1,)), ((), ()))


def nt(a, b):
    return lax.dot_general(a, b, NT, preferred_element_type=F32)


def nn(a, b):
    return jnp.dot(a, b, preferred_element_type=F32)


def eye(n):
    a = lax.broadcasted_iota(jnp.int32, (n, n), 0)
    b = lax.broadcasted_iota(jnp.int32, (n, n), 1)
    return (a == b).astype(F32).astype(BF16)


def kernel(
    zn,
    yn,
    tn,
    res_ref,
    qs_ref,
    ks_ref,
    vs_ref,
    ql_ref,
    kl_ref,
    vl_ref,
    fs_ref,
    fl_ref,
    wos_hbm,
    wol_hbm,
    gain_ref,
    wg_ref,
    wu_ref,
    cg_ref,
    cu_ref,
    wd_ref,
    out_ref,
    wos_ref,
    wol_ref,
    gat,
    gatz,
    ty,
    tz,
    wa,
    wb,
    cums,
    biass,
    biasl,
    edge,
    kks,
    kkl,
    vvs,
    vvl,
    accs,
    accl,
    stats,
    statl,
    oout,
    oin,
    sout,
    sin,
    fpo,
    fpi,
    dno,
    dni,
    first,
    ext,
    halo_out,
    halo_in,
    ebuf,
    hid,
    loc_s,
    gat_s,
    gat_r,
    t_s,
    t_r,
    w1_s,
    w1_r,
    w2_s,
    w2_r,
    o_s,
    o_r,
    st_s,
    st_r,
    fp_s,
    fp_r,
    n_s,
    n_r,
    d_s,
    d_r,
    h_s,
    h_r,
):
    sp = lax.axis_index("sp")
    tp = lax.axis_index("tp")
    z = sp // yn
    y = sp - z * yn
    tok = ks_ref.shape[0]
    wrows = wg_ref.shape[0]
    half = wa.shape[3]
    own = res_ref.shape[0]
    d = res_ref.shape[1]
    hy, hz = yn // 2, zn // 2
    sends = []

    def yid(dy):
        return (z * yn + lax.rem(y + dy + yn, yn), tp)

    def zid(dz):
        return (lax.rem(z + dz + zn, zn) * yn + y, tp)

    def tid(dt):
        return (sp, lax.rem(tp + dt, tn))

    def rc(src, dst, ss, rs, dev):
        return pltpu.make_async_remote_copy(
            src_ref=src, dst_ref=dst, send_sem=ss, recv_sem=rs, device_id=dev, device_id_type=MESH
        )

    def send(src, dst, ss, rs, dev):
        c = rc(src, dst, ss, rs, dev)
        c.start()
        sends.append(c)

    def landed(dst, ss, rs):
        rc(dst, dst, ss, rs, yid(1)).wait_recv()

    barrier = pltpu.get_barrier_semaphore()
    for i in range(1, yn):
        pl.semaphore_signal(barrier, inc=1, device_id=yid(i), device_id_type=MESH)
    for i in range(1, zn):
        pl.semaphore_signal(barrier, inc=1, device_id=zid(i), device_id_type=MESH)
    for i in range(1, tn):
        pl.semaphore_signal(barrier, inc=1, device_id=tid(i), device_id_type=MESH)

    @pl.when(sp > 0)
    def _():
        pl.semaphore_signal(barrier, inc=1, device_id=(sp - 1, tn - 1), device_id_type=MESH)

    loads = [
        pltpu.make_async_copy(wos_hbm, wos_ref, loc_s.at[0]),
        pltpu.make_async_copy(wol_hbm, wol_ref, loc_s.at[1]),
    ]
    for c in loads:
        c.start()

    def log_gate(x):
        u = jnp.exp(-jnp.abs(x))
        series = u * (1.0 - u * (0.5 - u * (1.0 / 3.0 - u * 0.25)))
        return jnp.minimum(x, 0.0) - jnp.where(u < 0.01, series, jnp.log(1.0 + u))

    row = jnp.concatenate(
        [log_gate(fs_ref[...]), log_gate(fl_ref[...]), jnp.zeros((5, tok), F32)], axis=0
    )
    lane = lax.broadcasted_iota(jnp.int32, row.shape, 1)
    shift = 1
    while shift < tok:
        row = row + jnp.where(lane >= shift, pltpu.roll(row, shift, 1), 0.0)
        shift *= 2
    gat[y] = row
    unit = eye(tok)
    ty[y, 0] = ks_ref[...]
    ty[y, 1] = nt(unit, vs_ref[...]).astype(BF16)
    ty[y, 2] = ql_ref[...]
    tz[z, 0] = kl_ref[...]
    tz[z, 1] = nt(unit, vl_ref[...]).astype(BF16)
    tz[z, 2] = qs_ref[...]
    for h, w in enumerate((wa, wb)):
        cols = slice(h * half, (h + 1) * half)
        w[z, y, 0:wrows] = wg_ref[:, cols]
        w[z, y, wrows : 2 * wrows] = wu_ref[:, cols]
        w[z, y, 2 * wrows : 3 * wrows] = wd_ref[:, cols]
    ext[0:16] = jnp.zeros((16, d), BF16)

    extra = jnp.where(jnp.logical_and(tp == tn - 1, sp < zn * yn - 1), tn, 0)
    pl.semaphore_wait(barrier, yn + zn + tn - 3 + extra)

    for i in range(1, yn):
        send(gat.at[y], gat.at[y], gat_s.at[0, i], gat_r.at[0, i], yid(i))

    def ring(axis, way, s, kind, start):
        n, me = (yn, y) if axis == 0 else (zn, z)
        k = way * (n // 2) + s - 1
        hop = s - 1 if start else s
        o = lax.rem(me + hop * (1 if way else -1) + n, n)
        last = s == n // 2
        if kind < 2:
            if last and kind != way:
                return
            ref = (ty if axis == 0 else tz).at[o, :, pl.ds(kind * (tok // 2), tok // 2)]
            ss, rs = t_s.at[axis, k, kind], t_r.at[axis, k, kind]
        else:
            ref = wa.at[z, o] if axis == 0 else wb.at[o, y]
            if last:
                step = 3 * wrows // 2
                ref = ref.at[pl.ds(way * step, step)]
            ss, rs = w1_s.at[axis, k], w1_r.at[axis, k]
        if start:
            send(ref, ref, ss, rs, (yid if axis == 0 else zid)(-1 if way else 1))
        else:
            landed(ref, ss, rs)

    def w2_part(axis, o, s, way, part):
        n, m = (zn, yn) if axis == 0 else (yn, zn)
        rows = pl.ds(0, 2 * wrows) if part == 0 else pl.ds(2 * wrows, wrows)
        if s < n // 2:
            span = pl.ds(0, m)
        else:
            span = pl.ds(way * (m // 2), m // 2)
        return wa.at[o, span, rows] if axis == 0 else wb.at[span, o, rows]

    def w2_send(axis, way, s, part):
        n, me = (zn, z) if axis == 0 else (yn, y)
        k = way * (n // 2) + s - 1
        o = lax.rem(me + (s - 1) * (1 if way else -1) + n, n)
        sl = w2_part(axis, o, s, way, part)
        to = (zid if axis == 0 else yid)(-1 if way else 1)
        send(sl, sl, w2_s.at[axis, k, part], w2_r.at[axis, k, part], to)

    def w2_wait(axis, way, s, part):
        n, me = (zn, z) if axis == 0 else (yn, y)
        k = way * (n // 2) + s - 1
        o = lax.rem(me + s * (1 if way else -1) + n, n)
        sl = w2_part(axis, o, s, way, part)
        landed(sl, w2_s.at[axis, k, part], w2_r.at[axis, k, part])

    def w2_step(s, part):
        for axis, n in ((0, zn), (1, yn)):
            for way in (0, 1):
                if 1 < s <= n // 2 + 1:
                    w2_wait(axis, way, s - 1, part)
                if s <= n // 2:
                    w2_send(axis, way, s, part)

    for kind in (0, 1, 2):
        for axis in (0, 1):
            for way in (0, 1):
                ring(axis, way, 1, kind, True)

    def ring_step(s, kinds):
        for kind in kinds:
            for axis, n in ((0, yn), (1, zn)):
                for way in (0, 1):
                    if s <= n // 2:
                        ring(axis, way, s, kind, False)
                    if s + 1 <= n // 2:
                        ring(axis, way, s + 1, kind, True)

    ring_step(1, (0, 1))
    for i in range(1, yn):
        landed(gat.at[lax.rem(y - i + yn, yn)], gat_s.at[0, i], gat_r.at[0, i])
    before = jnp.zeros((8, tok), F32)
    for i in range(yn):
        block = gat[i]
        cums[i] = (before + block) * LOG2E
        before = before + jnp.broadcast_to(block[:, tok - 1 : tok], block.shape)
    gatz[z, 0:8] = cums[y]
    gatz[z, 8:16] = before * LOG2E
    for i in range(1, zn):
        send(gatz.at[z], gatz.at[z], gat_s.at[1, i], gat_r.at[1, i], zid(i))
    ring_step(1, (2,))
    for i in range(yn):
        for h in range(2):
            column = -jnp.broadcast_to(cums[i, h : h + 1, :], (tok, tok)).T
            biass[h, i * tok : (i + 1) * tok] = column
    for s in range(2, max(hy, hz) + 1):
        ring_step(s, (0, 1, 2))
        if s == 2:
            for i in range(1, zn):
                landed(gatz.at[lax.rem(z - i + zn, zn)], gat_s.at[1, i], gat_r.at[1, i])
            gap = jnp.zeros((8, tok), F32)
            for i in reversed(range(zn)):
                gap = jnp.where(i < z, gap + gatz[i, 8:16], 0.0)
                away = jnp.where(i > z, -NEG, gatz[i, 2:3] - gap[2:3])
                column = -jnp.broadcast_to(away, (tok, tok)).T
                for j in range(2):
                    biasl[j, i * tok : (i + 1) * tok] = column
            edge[...] = -jnp.broadcast_to(gatz[z, 2:3], (tok, tok)).T

    w2_step(1, 0)
    w2_step(1, 1)
    key_lane = lax.broadcasted_iota(jnp.int32, (tok, 128), 1)
    for i in range(yn):
        rows = slice(i * tok, (i + 1) * tok)
        ksm = ty[i, 0]
        zero = jnp.zeros_like(ksm)
        kks[0, rows] = jnp.where(key_lane < 64, ksm, zero)
        kks[1, rows] = jnp.where(key_lane < 64, zero, ksm)
        vvs[:, rows] = ty[i, 1]
    for i in range(zn):
        rows = slice(i * tok, (i + 1) * tok)
        kkl[rows] = tz[i, 0]
        vvl[:, rows] = tz[i, 1]

    def soft(keys, queries, shifts, scale, values, limit):
        raw = nt(keys, queries)
        tops, dens, ps = [], [], []
        for j in range(2):
            s = raw[:, j * tok : (j + 1) * tok] * scale + shifts[j]
            if limit is not None and j == 0:
                spot = lax.broadcasted_iota(jnp.int32, s.shape, 0)
                s = jnp.where(spot <= limit, s, NEG)
            top = jnp.max(s, axis=0, keepdims=True)
            p = jnp.exp2(s - top)
            tops.append(top)
            dens.append(jnp.sum(p, axis=0, keepdims=True))
            ps.append(p.astype(BF16))
        return tops, dens, nn(values, jnp.concatenate(ps, axis=1))

    def two(ref, first_one, n):
        other = lax.rem(first_one + 1, n)
        return jnp.concatenate([ref[lax.rem(first_one, n), 2], ref[other, 2]], axis=0)

    def push(slot, i, to):
        rc(oout.at[slot, i], oin.at[slot, i], o_s.at[slot, i], o_r.at[slot, i], to).start()
        rc(sout.at[slot, i], sin.at[slot, i], st_s.at[slot, i], st_r.at[slot, i], to).start()

    def small(p, limit):
        queries = two(tz, z + 2 * p, zn)
        for h in range(2):
            lo, hi = 64 * h, 64 * h + 64
            shift = biass[h]
            tops, dens, part = soft(
                kks[h], queries, (shift, shift), 64 ** (-0.5) * LOG2E, vvs[lo:hi], limit
            )
            for j in range(2):
                piece = part[:, j * tok : (j + 1) * tok]
                if limit is not None and j == 0:
                    stats[0, h : h + 1] = tops[j]
                    stats[0, 2 + h : 3 + h] = dens[j]
                    accs[0, lo:hi] = piece
                else:
                    sout[0, 2 * p + j, h : h + 1] = tops[j]
                    sout[0, 2 * p + j, 2 + h : 3 + h] = dens[j]
                    oout[0, 2 * p + j, lo:hi] = piece.astype(BF16)
        for j in range(2):
            if limit is None or j == 1:

                @pl.when(z + 2 * p + j < zn)
                def _():
                    push(0, 2 * p + j, (sp + (2 * p + j) * yn, tp))

    def small_step(p, c):
        small(p, None)
        return c

    lax.fori_loop(1, (zn - z + 1) // 2, small_step, 0)
    small(0, y * tok + lax.broadcasted_iota(jnp.int32, (1, tok), 1))

    def large(p, c):
        a = lax.broadcasted_iota(jnp.int32, (tok, tok), 0)
        b = lax.broadcasted_iota(jnp.int32, (tok, tok), 1)
        rows = pl.ds(pl.multiple_of(z * tok, tok), tok)
        for j in range(2):
            o = lax.rem(y + 2 * p + j, yn)
            biasl[j, rows] = jnp.where(y * tok + a <= o * tok + b, edge[...], NEG)
        tops, dens, part = soft(
            kkl[...],
            two(ty, y + 2 * p, yn),
            (biasl[0], biasl[1]),
            128 ** (-0.5) * LOG2E,
            vvl[...],
            None,
        )
        for j in range(2):
            i = 2 * p + j
            o = lax.rem(y + i, yn)
            piece = part[:, j * tok : (j + 1) * tok]
            sout[1, i, 0:1] = tops[j]
            sout[1, i, 2:3] = dens[j]
            oout[1, i] = piece.astype(BF16)
            if j == 0:

                @pl.when(p == 0)
                def _():
                    statl[0, 0:1] = tops[0]
                    statl[0, 2:3] = dens[0]
                    accl[0] = piece

            @pl.when(jnp.logical_and(i > 0, jnp.logical_or(z > 0, o > y)))
            def _():
                push(1, i, (z * yn + o, tp))

        return c

    lax.fori_loop(0, yn // 2, large, 0)
    w2_step(2, 0)
    w2_step(2, 1)

    def fold(acc, stat, slot, lo, hi, i, row, gap):
        old = stat[0, row : row + 1]
        new = sin[slot, i, row : row + 1]
        if gap is not None:
            new = new + gap
        top = jnp.maximum(old, new)
        a = jnp.exp2(old - top)
        b = jnp.exp2(new - top)
        stat[0, row : row + 1] = top
        den = a * stat[0, 2 + row : 3 + row] + b * sin[slot, i, 2 + row : 3 + row]
        stat[0, 2 + row : 3 + row] = den
        acc[0, lo:hi] = a * acc[0, lo:hi] + b * oin[slot, i, lo:hi].astype(F32)

    def merge(i, gap):
        landed(oin.at[0, i], o_s.at[0, i], o_r.at[0, i])
        landed(sin.at[0, i], st_s.at[0, i], st_r.at[0, i])
        gap = gap + gatz[z - i, 8:16]
        for h in range(2):
            fold(accs, stats, 0, 64 * h, 64 * h + 64, i, h, gap[h : h + 1])
        return gap

    lax.fori_loop(1, z + 1, merge, jnp.zeros((8, tok), F32))

    def merge_large(i, c):
        @pl.when(jnp.logical_or(z > 0, lax.rem(y - i + yn, yn) < y))
        def _():
            landed(oin.at[1, i], o_s.at[1, i], o_r.at[1, i])
            landed(sin.at[1, i], st_s.at[1, i], st_r.at[1, i])
            fold(accl, statl, 1, 0, 128, i, 0, None)

        return c

    lax.fori_loop(1, yn, merge_large, 0)
    normed = []
    for h in range(3):
        if h < 2:
            att = accs[0, 64 * h : 64 * h + 64] / stats[0, 2 + h : 3 + h]
        else:
            att = accl[0] / statl[0, 2:3]
        mean = jnp.mean(att * att, axis=0, keepdims=True)
        normed.append(att * lax.rsqrt(mean + EPS))
    nsm = jnp.concatenate(normed[:2], axis=0).T.astype(BF16)
    nla = normed[2].T.astype(BF16)
    for c in loads:
        c.wait()
    width = min(512, d)
    for c in range(d // width):
        cols = slice(c * width, (c + 1) * width)
        fpo[:, cols] = (nn(nsm, wos_ref[:, cols]) + nn(nla, wol_ref[:, cols])).astype(BF16)

    def mine(ref, t):
        return ref.at[pl.ds(pl.multiple_of(t * own, own), own)]

    for i in range(1, tn):
        send(mine(fpo, lax.rem(tp + i, tn)), fpi.at[i], fp_s.at[i], fp_r.at[i], tid(i))
    w2_step(3, 0)
    value = res_ref[...].astype(F32) + mine(fpo, tp)[...].astype(F32)
    for i in range(1, tn):
        landed(fpi.at[i], fp_s.at[i], fp_r.at[i])
        value = value + fpi[i].astype(F32)
    first[...] = value
    mean = jnp.mean(value * value, axis=1, keepdims=True)
    normal = value * lax.rsqrt(mean + EPS) * gain_ref[...]
    place = ext.at[pl.ds(pl.multiple_of(16 + tp * own, 16), own)]
    place[...] = normal.astype(BF16)
    for i in range(1, tn):
        send(place, place, n_s.at[i], n_r.at[i], tid(i))
    hw = d // 8

    @pl.when(jnp.logical_and(tp == tn - 1, sp < zn * yn - 1))
    def _():
        rows = [normal[own - 2 : own, c * hw : (c + 1) * hw] for c in range(8)]
        halo_out[...] = jnp.concatenate(rows, axis=0).astype(BF16)
        for i in range(tn):
            rc(halo_out, halo_in, h_s.at[i], h_r, (sp + 1, i)).start()

    w2_step(3, 1)
    w2_step(4, 0)

    @pl.when(sp > 0)
    def _():
        landed(halo_in, h_s.at[0], h_r)
        block = halo_in[...].astype(F32)
        for c in range(8):
            pad = jnp.zeros((14, hw), F32)
            rim = jnp.concatenate([pad, block[2 * c : 2 * c + 2]], axis=0)
            ext[0:16, c * hw : (c + 1) * hw] = rim.astype(BF16)

    for i in range(1, tn):
        src = lax.rem(tp - i + tn, tn)
        landed(ext.at[pl.ds(pl.multiple_of(16 + src * own, 16), own)], n_s.at[i], n_r.at[i])
    w2_step(4, 1)
    w2_step(5, 0)

    count = zn * yn
    for h, (w, _n) in enumerate(((wa, 0), (wb, 1))):
        cols = slice(h * half, (h + 1) * half)
        conv = []
        for j, taps in ((0, cg_ref), (1, cu_ref)):
            weight = w[:, :, j * wrows : (j + 1) * wrows].reshape(count * wrows, half)
            ebuf[j] = nn(ext[...], weight).astype(BF16).astype(F32)
            conv.append(
                taps[0:1, cols] * ebuf[j, 14 : 14 + tok]
                + taps[1:2, cols] * ebuf[j, 15 : 15 + tok]
                + taps[2:3, cols] * ebuf[j, 16 : 16 + tok]
            )
        hid[h] = (conv[0] / (1.0 + jnp.exp(-conv[0])) * conv[1]).astype(BF16)

    w2_step(5, 1)
    zs = max(1, zn // 4)
    for c in range(zn // zs):
        span = zs * yn * wrows
        total_down = None
        for h, w in enumerate((wa, wb)):
            weight = w[c * zs : (c + 1) * zs, :, 2 * wrows : 3 * wrows].reshape(span, half)
            term = nt(hid[h], weight)
            total_down = term if total_down is None else total_down + term
        dno[:, c * span : (c + 1) * span] = total_down.astype(BF16)
    for i in range(1, tn):
        send(mine(dno, lax.rem(tp + i, tn)), dni.at[i], d_s.at[i], d_r.at[i], tid(i))
    value = first[...] + mine(dno, tp)[...].astype(F32)
    for i in range(1, tn):
        landed(dni.at[i], d_s.at[i], d_r.at[i])
        value = value + dni[i].astype(F32)
    out_ref[...] = value.astype(BF16)

    for c in sends:
        c.wait_send()
    for i in range(1, zn):

        @pl.when(z + i < zn)
        def _():
            rc(oout.at[0, i], oin.at[0, i], o_s.at[0, i], o_r.at[0, i], yid(1)).wait_send()
            rc(sout.at[0, i], sin.at[0, i], st_s.at[0, i], st_r.at[0, i], yid(1)).wait_send()

    for i in range(1, yn):

        @pl.when(jnp.logical_or(z > 0, lax.rem(y + i, yn) > y))
        def _():
            rc(oout.at[1, i], oin.at[1, i], o_s.at[1, i], o_r.at[1, i], yid(1)).wait_send()
            rc(sout.at[1, i], sin.at[1, i], st_s.at[1, i], st_r.at[1, i], yid(1)).wait_send()

    @pl.when(jnp.logical_and(tp == tn - 1, sp < zn * yn - 1))
    def _():
        for i in range(tn):
            rc(halo_out, halo_in, h_s.at[i], h_r, yid(1)).wait_send()


def body(
    sizes,
    residual,
    q_small,
    k_small,
    v_small,
    q_large,
    k_large,
    v_large,
    forget_small,
    forget_large,
    w_out_small,
    w_out_large,
    norm_gain,
    w_gate,
    w_up,
    conv_gate,
    conv_up,
    w_down,
):
    zn, yn, tn = sizes
    tok = q_small.shape[0]
    own, d = residual.shape
    wrows, ff = w_gate.shape
    half = ff // 2
    dma = pltpu.SemaphoreType.DMA
    big = max(yn, zn)
    scratch = [
        pltpu.VMEM(w_out_small.shape, BF16),
        pltpu.VMEM(w_out_large.shape, BF16),
        pltpu.VMEM((yn, 8, tok), F32),
        pltpu.VMEM((zn, 16, tok), F32),
        pltpu.VMEM((yn, 3, tok, 128), BF16),
        pltpu.VMEM((zn, 3, tok, 128), BF16),
        pltpu.VMEM((zn, yn, 3 * wrows, half), BF16),
        pltpu.VMEM((zn, yn, 3 * wrows, half), BF16),
        pltpu.VMEM((yn, 8, tok), F32),
        pltpu.VMEM((2, yn * tok, tok), F32),
        pltpu.VMEM((2, zn * tok, tok), F32),
        pltpu.VMEM((tok, tok), F32),
        pltpu.VMEM((2, yn * tok, 128), BF16),
        pltpu.VMEM((zn * tok, 128), BF16),
        pltpu.VMEM((128, yn * tok), BF16),
        pltpu.VMEM((128, zn * tok), BF16),
        pltpu.VMEM((1, 128, tok), F32),
        pltpu.VMEM((1, 128, tok), F32),
        pltpu.VMEM((1, 8, tok), F32),
        pltpu.VMEM((1, 8, tok), F32),
        pltpu.VMEM((2, big, 128, tok), BF16),
        pltpu.VMEM((2, big, 128, tok), BF16),
        pltpu.VMEM((2, big, 8, tok), F32),
        pltpu.VMEM((2, big, 8, tok), F32),
        pltpu.VMEM((tok, d), BF16),
        pltpu.VMEM((tn, own, d), BF16),
        pltpu.VMEM((tok, d), BF16),
        pltpu.VMEM((tn, own, d), BF16),
        pltpu.VMEM((own, d), F32),
        pltpu.VMEM((tok + 16, d), BF16),
        pltpu.VMEM((16, d // 8), BF16),
        pltpu.VMEM((16, d // 8), BF16),
        pltpu.VMEM((2, tok + 16, half), F32),
        pltpu.VMEM((2, tok, half), BF16),
        dma((2,)),
        dma((2, big)),
        dma((2, big)),
        dma((2, big, 2)),
        dma((2, big, 2)),
        dma((2, big)),
        dma((2, big)),
        dma((2, big, 2)),
        dma((2, big, 2)),
        dma((2, big)),
        dma((2, big)),
        dma((2, big)),
        dma((2, big)),
        dma((tn,)),
        dma((tn,)),
        dma((tn,)),
        dma((tn,)),
        dma((tn,)),
        dma((tn,)),
        dma((tn,)),
        dma,
    ]
    vmem = pl.BlockSpec(memory_space=pltpu.VMEM)
    hbm = pl.BlockSpec(memory_space=pl.ANY)
    return pl.pallas_call(
        functools.partial(kernel, zn, yn, tn),
        out_shape=jax.ShapeDtypeStruct((own, d), BF16),
        in_specs=[vmem] * 9 + [hbm] * 2 + [vmem] * 6,
        out_specs=pl.BlockSpec(memory_space=pltpu.VMEM),
        scratch_shapes=scratch,
        compiler_params=pltpu.CompilerParams(
            collective_id=0, has_side_effects=True, vmem_limit_bytes=60 * 1024 * 1024
        ),
    )(
        residual,
        q_small,
        k_small,
        v_small,
        q_large,
        k_large,
        v_large,
        forget_small.T,
        forget_large.T,
        w_out_small,
        w_out_large,
        norm_gain.reshape(1, d),
        w_gate,
        w_up,
        conv_gate,
        conv_up,
        w_down.T,
    )


def solution(mesh):
    sp = mesh.shape["sp"]
    yn = math.isqrt(sp)
    zn = sp // yn
    placed = (
        P(("sp", "tp"), None),
        P("sp", "tp"),
        P("sp", "tp"),
        P("sp", "tp"),
        P("sp", "tp"),
        P("sp", "tp"),
        P("sp", "tp"),
        P("sp", "tp"),
        P("sp", "tp"),
        P("tp", None),
        P("tp", None),
        P(),
        P("sp", "tp"),
        P("sp", "tp"),
        P(None, "tp"),
        P(None, "tp"),
        P("tp", "sp"),
    )
    return jax.shard_map(
        functools.partial(body, (zn, yn, mesh.shape["tp"])),
        mesh=mesh,
        in_specs=placed,
        out_specs=P(("sp", "tp"), None),
        check_vma=False,
    )
```

```python
import functools
import math

import jax
import jax.numpy as jnp
from jax import lax
from jax.experimental import pallas as pl
from jax.experimental.pallas import tpu as pltpu
from jax.sharding import PartitionSpec as P

EPS = 1e-06
NEG = -1e30
LOG2E = math.log2(math.e)
F32 = jnp.float32
BF16 = jnp.bfloat16
MESH = pl.DeviceIdType.MESH
NT = (((1,), (1,)), ((), ()))


def nt(a, b):
    return lax.dot_general(a, b, NT, preferred_element_type=F32)


def nn(a, b):
    return jnp.dot(a, b, preferred_element_type=F32)


def eye(n):
    a = lax.broadcasted_iota(jnp.int32, (n, n), 0)
    b = lax.broadcasted_iota(jnp.int32, (n, n), 1)
    return (a == b).astype(F32).astype(BF16)


def kernel(
    zn,
    yn,
    tn,
    res_hbm,
    qs_hbm,
    ks_hbm,
    vs_hbm,
    ql_hbm,
    kl_hbm,
    vl_hbm,
    fs_hbm,
    fl_hbm,
    wos_hbm,
    wol_hbm,
    gain_hbm,
    wg_hbm,
    wu_hbm,
    cg_hbm,
    cu_hbm,
    wd_hbm,
    out_ref,
    res_ref,
    qs_ref,
    ks_ref,
    vs_ref,
    ql_ref,
    kl_ref,
    vl_ref,
    fs_ref,
    fl_ref,
    wos_ref,
    wol_ref,
    gain_ref,
    wg_ref,
    wu_ref,
    cg_ref,
    cu_ref,
    wd_ref,
    gat,
    gatz,
    ty,
    tz,
    wa,
    wb,
    cums,
    biass,
    biasl,
    edge,
    kks,
    kkl,
    vvs,
    vvl,
    accs,
    accl,
    stats,
    statl,
    oout,
    oin,
    sout,
    sin,
    fpo,
    fpi,
    dno,
    dni,
    dnm,
    dnx,
    first,
    ext,
    halo_out,
    halo_in,
    ebuf,
    hid,
    loc_s,
    gat_s,
    gat_r,
    t_s,
    t_r,
    w1_s,
    w1_r,
    b_s,
    b_r,
    w2_s,
    w2_r,
    o_s,
    o_r,
    st_s,
    st_r,
    fp_s,
    fp_r,
    n_s,
    n_r,
    d_s,
    d_r,
    h_s,
    h_r,
):
    sp = lax.axis_index("sp")
    tp = lax.axis_index("tp")
    z = sp // yn
    y = sp - z * yn
    tok = ks_ref.shape[0]
    wrows = wg_ref.shape[0]
    half = wa.shape[3]
    own = res_ref.shape[0]
    d = res_ref.shape[1]
    hy, hz = yn // 2, zn // 2
    sends = []

    def yid(dy):
        return (z * yn + lax.rem(y + dy + yn, yn), tp)

    def zid(dz):
        return (lax.rem(z + dz + zn, zn) * yn + y, tp)

    def tid(dt):
        return (sp, lax.rem(tp + dt, tn))

    def rc(src, dst, ss, rs, dev):
        return pltpu.make_async_remote_copy(
            src_ref=src, dst_ref=dst, send_sem=ss, recv_sem=rs, device_id=dev, device_id_type=MESH
        )

    def send(src, dst, ss, rs, dev):
        c = rc(src, dst, ss, rs, dev)
        c.start()
        sends.append(c)

    def landed(dst, ss, rs):
        rc(dst, dst, ss, rs, yid(1)).wait_recv()

    inputs = (
        (res_hbm, res_ref),
        (qs_hbm, qs_ref),
        (ks_hbm, ks_ref),
        (vs_hbm, vs_ref),
        (ql_hbm, ql_ref),
        (kl_hbm, kl_ref),
        (vl_hbm, vl_ref),
        (fs_hbm, fs_ref),
        (fl_hbm, fl_ref),
        (gain_hbm, gain_ref),
        (wg_hbm, wg_ref),
        (wu_hbm, wu_ref),
        (cg_hbm, cg_ref),
        (cu_hbm, cu_ref),
        (wd_hbm, wd_ref),
        (wos_hbm, wos_ref),
        (wol_hbm, wol_ref),
    )
    loads = [pltpu.make_async_copy(a, b, loc_s.at[i]) for i, (a, b) in enumerate(inputs)]
    for c in loads:
        c.start()

    barrier = pltpu.get_barrier_semaphore()
    for i in range(1, yn):
        pl.semaphore_signal(barrier, inc=1, device_id=yid(i), device_id_type=MESH)
    for i in range(1, zn):
        pl.semaphore_signal(barrier, inc=1, device_id=zid(i), device_id_type=MESH)
    for i in range(1, tn):
        pl.semaphore_signal(barrier, inc=1, device_id=tid(i), device_id_type=MESH)

    @pl.when(sp > 0)
    def _():
        pl.semaphore_signal(barrier, inc=1, device_id=(sp - 1, tn - 1), device_id_type=MESH)

    for c in loads[:-2]:
        c.wait()

    def log_gate(x):
        u = jnp.exp(-jnp.abs(x))
        series = u * (1.0 - u * (0.5 - u * (1.0 / 3.0 - u * 0.25)))
        return jnp.minimum(x, 0.0) - jnp.where(u < 0.01, series, jnp.log(1.0 + u))

    row = jnp.concatenate(
        [log_gate(fs_ref[...]), log_gate(fl_ref[...]), jnp.zeros((5, tok), F32)], axis=0
    )
    lane = lax.broadcasted_iota(jnp.int32, row.shape, 1)
    shift = 1
    while shift < tok:
        row = row + jnp.where(lane >= shift, pltpu.roll(row, shift, 1), 0.0)
        shift *= 2
    gat[y] = row
    unit = eye(tok)
    ty[y, 0] = ks_ref[...]
    ty[y, 1] = nt(unit, vs_ref[...]).astype(BF16)
    ty[y, 2] = ql_ref[...]
    tz[z, 0] = kl_ref[...]
    tz[z, 1] = nt(unit, vl_ref[...]).astype(BF16)
    tz[z, 2] = qs_ref[...]
    for h, w in enumerate((wa, wb)):
        cols = slice(h * half, (h + 1) * half)
        w[z, y, 0:wrows] = wg_ref[:, cols]
        w[z, y, wrows : 2 * wrows] = wu_ref[:, cols]
        w[z, y, 2 * wrows : 3 * wrows] = wd_ref[:, cols]
    ext[0:16] = jnp.zeros((16, d), BF16)

    extra = jnp.where(jnp.logical_and(tp == tn - 1, sp < zn * yn - 1), tn, 0)
    pl.semaphore_wait(barrier, yn + zn + tn - 3 + extra)

    for i in range(1, yn):
        send(gat.at[y], gat.at[y], gat_s.at[0, i], gat_r.at[0, i], yid(i))

    def ring(axis, way, s, kind, start):
        n, me = (yn, y) if axis == 0 else (zn, z)
        k = way * (n // 2) + s - 1
        hop = s - 1 if start else s
        o = lax.rem(me + hop * (1 if way else -1) + n, n)
        last = s == n // 2
        if kind < 2:
            if last and kind != way:
                return
            ref = (ty if axis == 0 else tz).at[o, :, pl.ds(kind * (tok // 2), tok // 2)]
            ss, rs = t_s.at[axis, k, kind], t_r.at[axis, k, kind]
        else:
            ref = wa.at[z, o] if axis == 0 else wb.at[o, y]
            if last:
                step = 3 * wrows // 2
                ref = ref.at[pl.ds(way * step, step)]
            ss, rs = w1_s.at[axis, k], w1_r.at[axis, k]
        if start:
            send(ref, ref, ss, rs, (yid if axis == 0 else zid)(-1 if way else 1))
        else:
            landed(ref, ss, rs)

    def w2_part(axis, o, s, way, part):
        n, m = (zn, yn) if axis == 0 else (yn, zn)
        rows = pl.ds(0, 2 * wrows) if part == 0 else pl.ds(2 * wrows, wrows)
        if s < n // 2:
            span = pl.ds(0, m)
        else:
            span = pl.ds(way * (m // 2), m // 2)
        return wa.at[o, span, rows] if axis == 0 else wb.at[span, o, rows]

    def w2_send(axis, way, s, part):
        n, me = (zn, z) if axis == 0 else (yn, y)
        k = way * (n // 2) + s - 1
        o = lax.rem(me + (s - 1) * (1 if way else -1) + n, n)
        sl = w2_part(axis, o, s, way, part)
        to = (zid if axis == 0 else yid)(-1 if way else 1)
        send(sl, sl, w2_s.at[axis, k, part], w2_r.at[axis, k, part], to)

    def w2_wait(axis, way, s, part):
        n, me = (zn, z) if axis == 0 else (yn, y)
        k = way * (n // 2) + s - 1
        o = lax.rem(me + s * (1 if way else -1) + n, n)
        sl = w2_part(axis, o, s, way, part)
        landed(sl, w2_s.at[axis, k, part], w2_r.at[axis, k, part])

    def hop(axis, g, start):
        m, me, pos = (yn, z, y) if axis == 0 else (zn, y, z)
        n = zn if axis == 0 else yn
        b = lax.rem(pos + g + m, m)
        for way in (0, 1):
            o = me if start else lax.rem(me + (1 if way else -1) + n, n)
            ref = wa.at[o, b] if axis == 0 else wb.at[b, o]
            ss, rs = b_s.at[axis, way, g % m], b_r.at[axis, way, g % m]
            if start:
                send(ref, ref, ss, rs, (zid if axis == 0 else yid)(-1 if way else 1))
            else:
                landed(ref, ss, rs)

    def w2_step(s, part):
        for axis, n in ((0, zn), (1, yn)):
            m = yn if axis == 0 else zn
            if s == 2 and part == 0:
                for g in range(m):
                    hop(axis, g, False)
            for way in (0, 1):
                if 2 < s <= n // 2 + 1:
                    w2_wait(axis, way, s - 1, part)
                if s <= n // 2:
                    w2_send(axis, way, s, part)

    for kind in (0, 1, 2):
        for axis in (0, 1):
            for way in (0, 1):
                ring(axis, way, 1, kind, True)
    hop(0, 0, True)
    hop(1, 0, True)

    def ring_step(s, kinds):
        for kind in kinds:
            for axis, n in ((0, yn), (1, zn)):
                for way in (0, 1):
                    if s <= n // 2:
                        ring(axis, way, s, kind, False)
                    if s + 1 <= n // 2:
                        ring(axis, way, s + 1, kind, True)

    ring_step(1, (0, 1))
    for i in range(1, yn):
        landed(gat.at[lax.rem(y - i + yn, yn)], gat_s.at[0, i], gat_r.at[0, i])
    before = jnp.zeros((8, tok), F32)
    for i in range(yn):
        block = gat[i]
        cums[i] = (before + block) * LOG2E
        before = before + jnp.broadcast_to(block[:, tok - 1 : tok], block.shape)
    gatz[z, 0:8] = cums[y]
    gatz[z, 8:16] = before * LOG2E
    for i in range(1, zn):
        send(gatz.at[z], gatz.at[z], gat_s.at[1, i], gat_r.at[1, i], zid(i))
    ring_step(1, (2,))
    for i in range(yn):
        for h in range(2):
            column = -jnp.broadcast_to(cums[i, h : h + 1, :], (tok, tok)).T
            biass[h, i * tok : (i + 1) * tok] = column
    for s in range(2, max(hy, hz) + 1):
        ring_step(s, (0, 1, 2))
        for axis, m in ((0, yn), (1, zn)):
            if s == 2 and m > 2:
                hop(axis, -1, True)
            if s == 3 and m > 2:
                hop(axis, 1, True)
        if s == 2:
            for i in range(1, zn):
                landed(gatz.at[lax.rem(z - i + zn, zn)], gat_s.at[1, i], gat_r.at[1, i])
            gap = jnp.zeros((8, tok), F32)
            for i in reversed(range(zn)):
                gap = jnp.where(i < z, gap + gatz[i, 8:16], 0.0)
                away = jnp.where(i > z, -NEG, gatz[i, 2:3] - gap[2:3])
                column = -jnp.broadcast_to(away, (tok, tok)).T
                for j in range(2):
                    biasl[j, i * tok : (i + 1) * tok] = column
            edge[...] = -jnp.broadcast_to(gatz[z, 2:3], (tok, tok)).T

    for axis, m in ((0, yn), (1, zn)):
        for g in range(1, m):
            if g not in (1, m - 1) or m == 2:
                hop(axis, g, True)
    key_lane = lax.broadcasted_iota(jnp.int32, (tok, 128), 1)
    for i in range(yn):
        rows = slice(i * tok, (i + 1) * tok)
        ksm = ty[i, 0]
        zero = jnp.zeros_like(ksm)
        kks[0, rows] = jnp.where(key_lane < 64, ksm, zero)
        kks[1, rows] = jnp.where(key_lane < 64, zero, ksm)
        vvs[:, rows] = ty[i, 1]
    for i in range(zn):
        rows = slice(i * tok, (i + 1) * tok)
        kkl[rows] = tz[i, 0]
        vvl[:, rows] = tz[i, 1]

    def soft(keys, queries, shifts, scale, values, limit):
        raw = nt(keys, queries)
        tops, dens, ps = [], [], []
        for j in range(2):
            s = raw[:, j * tok : (j + 1) * tok] * scale + shifts[j]
            if limit is not None and j == 0:
                spot = lax.broadcasted_iota(jnp.int32, s.shape, 0)
                s = jnp.where(spot <= limit, s, NEG)
            top = jnp.max(s, axis=0, keepdims=True)
            p = jnp.exp2(s - top)
            tops.append(top)
            dens.append(jnp.sum(p, axis=0, keepdims=True))
            ps.append(p.astype(BF16))
        return tops, dens, nn(values, jnp.concatenate(ps, axis=1))

    def two(ref, first_one, n):
        other = lax.rem(first_one + 1, n)
        return jnp.concatenate([ref[lax.rem(first_one, n), 2], ref[other, 2]], axis=0)

    def push(slot, i, to):
        rc(oout.at[slot, i], oin.at[slot, i], o_s.at[slot, i], o_r.at[slot, i], to).start()
        rc(sout.at[slot, i], sin.at[slot, i], st_s.at[slot, i], st_r.at[slot, i], to).start()

    def small(p, limit):
        queries = two(tz, z + 2 * p, zn)
        for h in range(2):
            lo, hi = 64 * h, 64 * h + 64
            shift = biass[h]
            tops, dens, part = soft(
                kks[h], queries, (shift, shift), 64 ** (-0.5) * LOG2E, vvs[lo:hi], limit
            )
            for j in range(2):
                piece = part[:, j * tok : (j + 1) * tok]
                if limit is not None and j == 0:
                    stats[0, h : h + 1] = tops[j]
                    stats[0, 2 + h : 3 + h] = dens[j]
                    accs[0, lo:hi] = piece
                else:
                    sout[0, 2 * p + j, h : h + 1] = tops[j]
                    sout[0, 2 * p + j, 2 + h : 3 + h] = dens[j]
                    oout[0, 2 * p + j, lo:hi] = piece.astype(BF16)
        for j in range(2):
            if limit is None or j == 1:

                @pl.when(z + 2 * p + j < zn)
                def _():
                    push(0, 2 * p + j, (sp + (2 * p + j) * yn, tp))

    def small_step(p, c):
        small(p, None)
        return c

    def large(p, c):
        a = lax.broadcasted_iota(jnp.int32, (tok, tok), 0)
        b = lax.broadcasted_iota(jnp.int32, (tok, tok), 1)
        rows = pl.ds(pl.multiple_of(z * tok, tok), tok)
        for j in range(2):
            o = lax.rem(y + 2 * p + j, yn)
            biasl[j, rows] = jnp.where(y * tok + a <= o * tok + b, edge[...], NEG)
        tops, dens, part = soft(
            kkl[...],
            two(ty, y + 2 * p, yn),
            (biasl[0], biasl[1]),
            128 ** (-0.5) * LOG2E,
            vvl[...],
            None,
        )
        for j in range(2):
            i = 2 * p + j
            o = lax.rem(y + i, yn)
            piece = part[:, j * tok : (j + 1) * tok]
            sout[1, i, 0:1] = tops[j]
            sout[1, i, 2:3] = dens[j]
            oout[1, i] = piece.astype(BF16)
            if j == 0:

                @pl.when(p == 0)
                def _():
                    statl[0, 0:1] = tops[0]
                    statl[0, 2:3] = dens[0]
                    accl[0] = piece

            @pl.when(jnp.logical_and(i > 0, jnp.logical_or(z > 0, o > y)))
            def _():
                push(1, i, (z * yn + o, tp))

        return c

    lax.fori_loop(0, yn // 2, large, 0)
    lax.fori_loop(1, (zn - z + 1) // 2, small_step, 0)
    small(0, y * tok + lax.broadcasted_iota(jnp.int32, (1, tok), 1))

    w2_step(2, 0)
    w2_step(2, 1)

    def fold(acc, stat, slot, lo, hi, i, row, gap):
        old = stat[0, row : row + 1]
        new = sin[slot, i, row : row + 1]
        if gap is not None:
            new = new + gap
        top = jnp.maximum(old, new)
        a = jnp.exp2(old - top)
        b = jnp.exp2(new - top)
        stat[0, row : row + 1] = top
        den = a * stat[0, 2 + row : 3 + row] + b * sin[slot, i, 2 + row : 3 + row]
        stat[0, 2 + row : 3 + row] = den
        acc[0, lo:hi] = a * acc[0, lo:hi] + b * oin[slot, i, lo:hi].astype(F32)

    def merge(i, gap):
        landed(oin.at[0, i], o_s.at[0, i], o_r.at[0, i])
        landed(sin.at[0, i], st_s.at[0, i], st_r.at[0, i])
        gap = gap + gatz[z - i, 8:16]
        for h in range(2):
            fold(accs, stats, 0, 64 * h, 64 * h + 64, i, h, gap[h : h + 1])
        return gap

    lax.fori_loop(1, z + 1, merge, jnp.zeros((8, tok), F32))

    def merge_large(i, c):
        @pl.when(jnp.logical_or(z > 0, lax.rem(y - i + yn, yn) < y))
        def _():
            landed(oin.at[1, i], o_s.at[1, i], o_r.at[1, i])
            landed(sin.at[1, i], st_s.at[1, i], st_r.at[1, i])
            fold(accl, statl, 1, 0, 128, i, 0, None)

        return c

    lax.fori_loop(1, yn, merge_large, 0)
    normed = []
    for h in range(3):
        if h < 2:
            att = accs[0, 64 * h : 64 * h + 64] / stats[0, 2 + h : 3 + h]
        else:
            att = accl[0] / statl[0, 2:3]
        mean = jnp.mean(att * att, axis=0, keepdims=True)
        normed.append(att * lax.rsqrt(mean + EPS))
    nsm = jnp.concatenate(normed[:2], axis=0).T.astype(BF16)
    nla = normed[2].T.astype(BF16)
    for c in loads[-2:]:
        c.wait()
    width = min(512, d)
    for c in range(d // width):
        cols = slice(c * width, (c + 1) * width)
        fpo[:, cols] = (nn(nsm, wos_ref[:, cols]) + nn(nla, wol_ref[:, cols])).astype(BF16)

    def mine(ref, t):
        return ref.at[pl.ds(pl.multiple_of(t * own, own), own)]

    for i in range(1, tn):
        send(mine(fpo, lax.rem(tp + i, tn)), fpi.at[i], fp_s.at[i], fp_r.at[i], tid(i))
    w2_step(3, 0)
    value = res_ref[...].astype(F32) + mine(fpo, tp)[...].astype(F32)
    for i in range(1, tn):
        landed(fpi.at[i], fp_s.at[i], fp_r.at[i])
        value = value + fpi[i].astype(F32)
    first[...] = value
    mean = jnp.mean(value * value, axis=1, keepdims=True)
    normal = value * lax.rsqrt(mean + EPS) * gain_ref[...]
    place = ext.at[pl.ds(pl.multiple_of(16 + tp * own, 16), own)]
    place[...] = normal.astype(BF16)
    for i in range(1, tn):
        send(place, place, n_s.at[i], n_r.at[i], tid(i))
    hw = d // 8

    @pl.when(jnp.logical_and(tp == tn - 1, sp < zn * yn - 1))
    def _():
        rows = [normal[own - 2 : own, c * hw : (c + 1) * hw] for c in range(8)]
        halo_out[...] = jnp.concatenate(rows, axis=0).astype(BF16)
        for i in range(tn):
            rc(halo_out, halo_in, h_s.at[i], h_r, (sp + 1, i)).start()

    w2_step(3, 1)
    w2_step(4, 0)

    @pl.when(sp > 0)
    def _():
        landed(halo_in, h_s.at[0], h_r)
        block = halo_in[...].astype(F32)
        for c in range(8):
            pad = jnp.zeros((14, hw), F32)
            rim = jnp.concatenate([pad, block[2 * c : 2 * c + 2]], axis=0)
            ext[0:16, c * hw : (c + 1) * hw] = rim.astype(BF16)

    for i in range(1, tn):
        src = lax.rem(tp - i + tn, tn)
        landed(ext.at[pl.ds(pl.multiple_of(16 + src * own, 16), own)], n_s.at[i], n_r.at[i])
    w2_step(4, 1)
    w2_step(5, 0)

    count = zn * yn
    for h, (w, _n) in enumerate(((wa, 0), (wb, 1))):
        cols = slice(h * half, (h + 1) * half)
        conv = []
        for j, taps in ((0, cg_ref), (1, cu_ref)):
            weight = w[:, :, j * wrows : (j + 1) * wrows].reshape(count * wrows, half)
            ebuf[j] = nn(ext[...], weight).astype(BF16).astype(F32)
            conv.append(
                taps[0:1, cols] * ebuf[j, 14 : 14 + tok]
                + taps[1:2, cols] * ebuf[j, 15 : 15 + tok]
                + taps[2:3, cols] * ebuf[j, 16 : 16 + tok]
            )
        hid[h] = (conv[0] / (1.0 + jnp.exp(-conv[0])) * conv[1]).astype(BF16)

    w2_step(5, 1)
    zs = max(1, zn // 4)
    for c in range(zn // zs):
        span = zs * yn * wrows
        total_down = None
        for h, w in enumerate((wa, wb)):
            weight = w[c * zs : (c + 1) * zs, :, 2 * wrows : 3 * wrows].reshape(span, half)
            term = nt(hid[h], weight)
            total_down = term if total_down is None else total_down + term
        dno[:, :, :, c * span : (c + 1) * span] = total_down.astype(BF16).reshape(
            tn // 2, 2, own, span
        )
    core = lax.rem(tp, 2)
    mate = (sp, tp + 1 - 2 * core)
    pairs = tn // 2
    spot = tp // 2
    send(dno.at[:, 1 - core], dnm, d_s.at[0], d_r.at[0], mate)
    landed(dnm, d_s.at[0], d_r.at[0])
    for i in range(1, pairs):
        k = lax.rem(spot + i, pairs)
        dnx[i] = (dno[k, core].astype(F32) + dnm[k].astype(F32)).astype(BF16)
        send(dnx.at[i], dni.at[i], d_s.at[i], d_r.at[i], (sp, 2 * k + core))
    value = first[...] + dno[spot, core].astype(F32) + dnm[spot].astype(F32)
    for i in range(1, pairs):
        landed(dni.at[i], d_s.at[i], d_r.at[i])
        value = value + dni[i].astype(F32)
    out_ref[...] = value

    for c in sends:
        c.wait_send()
    for i in range(1, zn):

        @pl.when(z + i < zn)
        def _():
            rc(oout.at[0, i], oin.at[0, i], o_s.at[0, i], o_r.at[0, i], yid(1)).wait_send()
            rc(sout.at[0, i], sin.at[0, i], st_s.at[0, i], st_r.at[0, i], yid(1)).wait_send()

    for i in range(1, yn):

        @pl.when(jnp.logical_or(z > 0, lax.rem(y + i, yn) > y))
        def _():
            rc(oout.at[1, i], oin.at[1, i], o_s.at[1, i], o_r.at[1, i], yid(1)).wait_send()
            rc(sout.at[1, i], sin.at[1, i], st_s.at[1, i], st_r.at[1, i], yid(1)).wait_send()

    @pl.when(jnp.logical_and(tp == tn - 1, sp < zn * yn - 1))
    def _():
        for i in range(tn):
            rc(halo_out, halo_in, h_s.at[i], h_r, yid(1)).wait_send()


def body(
    sizes,
    residual,
    q_small,
    k_small,
    v_small,
    q_large,
    k_large,
    v_large,
    forget_small,
    forget_large,
    w_out_small,
    w_out_large,
    norm_gain,
    w_gate,
    w_up,
    conv_gate,
    conv_up,
    w_down,
):
    zn, yn, tn = sizes
    tok = q_small.shape[0]
    own, d = residual.shape
    wrows, ff = w_gate.shape
    half = ff // 2
    operands = (
        residual,
        q_small,
        k_small,
        v_small,
        q_large,
        k_large,
        v_large,
        forget_small.T,
        forget_large.T,
        w_out_small,
        w_out_large,
        norm_gain.reshape(1, d),
        w_gate,
        w_up,
        conv_gate,
        conv_up,
        w_down.T,
    )
    dma = pltpu.SemaphoreType.DMA
    big = max(yn, zn)
    scratch = [
        *(pltpu.VMEM(a.shape, a.dtype) for a in operands),
        pltpu.VMEM((yn, 8, tok), F32),
        pltpu.VMEM((zn, 16, tok), F32),
        pltpu.VMEM((yn, 3, tok, 128), BF16),
        pltpu.VMEM((zn, 3, tok, 128), BF16),
        pltpu.VMEM((zn, yn, 3 * wrows, half), BF16),
        pltpu.VMEM((zn, yn, 3 * wrows, half), BF16),
        pltpu.VMEM((yn, 8, tok), F32),
        pltpu.VMEM((2, yn * tok, tok), F32),
        pltpu.VMEM((2, zn * tok, tok), F32),
        pltpu.VMEM((tok, tok), F32),
        pltpu.VMEM((2, yn * tok, 128), BF16),
        pltpu.VMEM((zn * tok, 128), BF16),
        pltpu.VMEM((128, yn * tok), BF16),
        pltpu.VMEM((128, zn * tok), BF16),
        pltpu.VMEM((1, 128, tok), F32),
        pltpu.VMEM((1, 128, tok), F32),
        pltpu.VMEM((1, 8, tok), F32),
        pltpu.VMEM((1, 8, tok), F32),
        pltpu.VMEM((2, big, 128, tok), BF16),
        pltpu.VMEM((2, big, 128, tok), BF16),
        pltpu.VMEM((2, big, 8, tok), F32),
        pltpu.VMEM((2, big, 8, tok), F32),
        pltpu.VMEM((tok, d), BF16),
        pltpu.VMEM((tn, own, d), BF16),
        pltpu.VMEM((tn // 2, 2, own, d), BF16),
        pltpu.VMEM((tn // 2, own, d), BF16),
        pltpu.VMEM((tn // 2, own, d), BF16),
        pltpu.VMEM((tn // 2, own, d), BF16),
        pltpu.VMEM((own, d), F32),
        pltpu.VMEM((tok + 16, d), BF16),
        pltpu.VMEM((16, d // 8), BF16),
        pltpu.VMEM((16, d // 8), BF16),
        pltpu.VMEM((2, tok + 16, half), F32),
        pltpu.VMEM((2, tok, half), BF16),
        dma((len(operands),)),
        dma((2, big)),
        dma((2, big)),
        dma((2, big, 2)),
        dma((2, big, 2)),
        dma((2, big)),
        dma((2, big)),
        dma((2, 2, big)),
        dma((2, 2, big)),
        dma((2, big, 2)),
        dma((2, big, 2)),
        dma((2, big)),
        dma((2, big)),
        dma((2, big)),
        dma((2, big)),
        dma((tn,)),
        dma((tn,)),
        dma((tn,)),
        dma((tn,)),
        dma((tn,)),
        dma((tn,)),
        dma((tn,)),
        dma,
    ]
    vmem = pl.BlockSpec(memory_space=pltpu.VMEM)
    hbm = pl.BlockSpec(memory_space=pl.ANY)
    result = pl.pallas_call(
        functools.partial(kernel, zn, yn, tn),
        out_shape=jax.ShapeDtypeStruct((own, d), F32),
        in_specs=[hbm] * len(operands),
        out_specs=pl.BlockSpec(memory_space=pltpu.VMEM),
        scratch_shapes=scratch,
        compiler_params=pltpu.CompilerParams(
            collective_id=0, has_side_effects=True, vmem_limit_bytes=60 * 1024 * 1024
        ),
    )(*operands)
    return result.astype(BF16)


def solution(mesh):
    sp = mesh.shape["sp"]
    yn = math.isqrt(sp)
    zn = sp // yn
    placed = (
        P(("sp", "tp"), None),
        P("sp", "tp"),
        P("sp", "tp"),
        P("sp", "tp"),
        P("sp", "tp"),
        P("sp", "tp"),
        P("sp", "tp"),
        P("sp", "tp"),
        P("sp", "tp"),
        P("tp", None),
        P("tp", None),
        P(),
        P("sp", "tp"),
        P("sp", "tp"),
        P(None, "tp"),
        P(None, "tp"),
        P("tp", "sp"),
    )
    return jax.shard_map(
        functools.partial(body, (zn, yn, mesh.shape["tp"])),
        mesh=mesh,
        in_specs=placed,
        out_specs=P(("sp", "tp"), None),
        check_vma=False,
    )
```

```python
import functools
import math

import jax
import jax.numpy as jnp
from jax import lax
from jax.experimental import pallas as pl
from jax.experimental.pallas import tpu as pltpu
from jax.sharding import PartitionSpec as P

EPS = 1e-06
NEG = -1e30
LOG2E = math.log2(math.e)
F32 = jnp.float32
BF16 = jnp.bfloat16
MESH = pl.DeviceIdType.MESH
NT = (((1,), (1,)), ((), ()))


def nt(a, b):
    return lax.dot_general(a, b, NT, preferred_element_type=F32)


def nn(a, b):
    return jnp.dot(a, b, preferred_element_type=F32)


def eye(n):
    a = lax.broadcasted_iota(jnp.int32, (n, n), 0)
    b = lax.broadcasted_iota(jnp.int32, (n, n), 1)
    return (a == b).astype(F32).astype(BF16)


def kernel(
    zn,
    yn,
    tn,
    res_hbm,
    qs_hbm,
    ks_hbm,
    vs_hbm,
    ql_hbm,
    kl_hbm,
    vl_hbm,
    fs_hbm,
    fl_hbm,
    wos_hbm,
    wol_hbm,
    gain_hbm,
    wg_hbm,
    wu_hbm,
    cg_hbm,
    cu_hbm,
    wd_hbm,
    out_ref,
    res_ref,
    qs_ref,
    ks_ref,
    vs_ref,
    ql_ref,
    kl_ref,
    vl_ref,
    fs_ref,
    fl_ref,
    wos_ref,
    wol_ref,
    gain_ref,
    wg_ref,
    wu_ref,
    cg_ref,
    cu_ref,
    wd_ref,
    gat,
    gatz,
    ty,
    tz,
    wa,
    wb,
    cums,
    biass,
    biasl,
    edge,
    kks,
    kkl,
    vvs,
    vvl,
    accs,
    accl,
    stats,
    statl,
    oout,
    oin,
    sout,
    sin,
    fpo,
    fpi,
    dno,
    dni,
    dnm,
    dnx,
    first,
    ext,
    halo_out,
    halo_in,
    ebuf,
    hid,
    loc_s,
    gat_s,
    gat_r,
    t_s,
    t_r,
    w1_s,
    w1_r,
    b_s,
    b_r,
    w2_s,
    w2_r,
    o_s,
    o_r,
    st_s,
    st_r,
    fp_s,
    fp_r,
    n_s,
    n_r,
    d_s,
    d_r,
    h_s,
    h_r,
):
    sp = lax.axis_index("sp")
    tp = lax.axis_index("tp")
    z = sp // yn
    y = sp - z * yn
    tok = ks_ref.shape[0]
    wrows = wg_ref.shape[0]
    half = wa.shape[3]
    own = res_ref.shape[0]
    d = res_ref.shape[1]
    hy, hz = yn // 2, zn // 2
    sends = []

    def yid(dy):
        return (z * yn + lax.rem(y + dy + yn, yn), tp)

    def zid(dz):
        return (lax.rem(z + dz + zn, zn) * yn + y, tp)

    def tid(dt):
        return (sp, lax.rem(tp + dt, tn))

    def rc(src, dst, ss, rs, dev):
        return pltpu.make_async_remote_copy(
            src_ref=src, dst_ref=dst, send_sem=ss, recv_sem=rs, device_id=dev, device_id_type=MESH
        )

    def send(src, dst, ss, rs, dev):
        c = rc(src, dst, ss, rs, dev)
        c.start()
        sends.append(c)

    def landed(dst, ss, rs):
        rc(dst, dst, ss, rs, yid(1)).wait_recv()

    inputs = (
        (res_hbm, res_ref),
        (qs_hbm, qs_ref),
        (ks_hbm, ks_ref),
        (vs_hbm, vs_ref),
        (ql_hbm, ql_ref),
        (kl_hbm, kl_ref),
        (vl_hbm, vl_ref),
        (fs_hbm, fs_ref),
        (fl_hbm, fl_ref),
        (gain_hbm, gain_ref),
        (wg_hbm, wg_ref),
        (wu_hbm, wu_ref),
        (cg_hbm, cg_ref),
        (cu_hbm, cu_ref),
        (wd_hbm, wd_ref),
        (wos_hbm, wos_ref),
        (wol_hbm, wol_ref),
    )
    loads = [pltpu.make_async_copy(a, b, loc_s.at[i]) for i, (a, b) in enumerate(inputs)]
    for c in loads:
        c.start()

    barrier = pltpu.get_barrier_semaphore()
    for i in range(1, yn):
        pl.semaphore_signal(barrier, inc=1, device_id=yid(i), device_id_type=MESH)
    for i in range(1, zn):
        pl.semaphore_signal(barrier, inc=1, device_id=zid(i), device_id_type=MESH)
    for i in range(1, tn):
        pl.semaphore_signal(barrier, inc=1, device_id=tid(i), device_id_type=MESH)

    @pl.when(sp > 0)
    def _():
        pl.semaphore_signal(barrier, inc=1, device_id=(sp - 1, tn - 1), device_id_type=MESH)

    for c in loads[:-2]:
        c.wait()

    def log_gate(x):
        u = jnp.exp(-jnp.abs(x))
        series = u * (1.0 - u * (0.5 - u * (1.0 / 3.0 - u * 0.25)))
        return jnp.minimum(x, 0.0) - jnp.where(u < 0.01, series, jnp.log(1.0 + u))

    row = jnp.concatenate(
        [log_gate(fs_ref[...]), log_gate(fl_ref[...]), jnp.zeros((5, tok), F32)], axis=0
    )
    lane = lax.broadcasted_iota(jnp.int32, row.shape, 1)
    shift = 1
    while shift < tok:
        row = row + jnp.where(lane >= shift, pltpu.roll(row, shift, 1), 0.0)
        shift *= 2
    gat[y] = row
    unit = eye(tok)
    ty[y, 0] = ks_ref[...]
    ty[y, 1] = nt(unit, vs_ref[...]).astype(BF16)
    ty[y, 2] = ql_ref[...]
    tz[z, 0] = kl_ref[...]
    tz[z, 1] = nt(unit, vl_ref[...]).astype(BF16)
    tz[z, 2] = qs_ref[...]
    for h, w in enumerate((wa, wb)):
        cols = slice(h * half, (h + 1) * half)
        w[z, y, 0:wrows] = wg_ref[:, cols]
        w[z, y, wrows : 2 * wrows] = wu_ref[:, cols]
        w[z, y, 2 * wrows : 3 * wrows] = wd_ref[:, cols]
    ext[0:16] = jnp.zeros((16, d), BF16)

    extra = jnp.where(jnp.logical_and(tp == tn - 1, sp < zn * yn - 1), tn, 0)
    pl.semaphore_wait(barrier, yn + zn + tn - 3 + extra)

    for i in range(1, yn):
        send(gat.at[y], gat.at[y], gat_s.at[0, i], gat_r.at[0, i], yid(i))

    def ring(axis, way, s, kind, start):
        n, me = (yn, y) if axis == 0 else (zn, z)
        k = way * (n // 2) + s - 1
        hop = s - 1 if start else s
        o = lax.rem(me + hop * (1 if way else -1) + n, n)
        last = s == n // 2
        if kind < 2:
            if last and kind != way:
                return
            ref = (ty if axis == 0 else tz).at[o, :, pl.ds(kind * (tok // 2), tok // 2)]
            ss, rs = t_s.at[axis, k, kind], t_r.at[axis, k, kind]
        else:
            ref = wa.at[z, o] if axis == 0 else wb.at[o, y]
            if last:
                step = 3 * wrows // 2
                ref = ref.at[pl.ds(way * step, step)]
            ss, rs = w1_s.at[axis, k], w1_r.at[axis, k]
        if start:
            send(ref, ref, ss, rs, (yid if axis == 0 else zid)(-1 if way else 1))
        else:
            landed(ref, ss, rs)

    def w2_part(axis, o, s, way, part):
        n, m = (zn, yn) if axis == 0 else (yn, zn)
        rows = pl.ds(0, 2 * wrows) if part == 0 else pl.ds(2 * wrows, wrows)
        if s < n // 2:
            span = pl.ds(0, m)
        else:
            cut = max(1, 2 * m // 8)
            span = pl.ds(cut, m - cut) if way else pl.ds(0, cut)
        return wa.at[o, span, rows] if axis == 0 else wb.at[span, o, rows]

    def w2_send(axis, way, s, part):
        n, me = (zn, z) if axis == 0 else (yn, y)
        k = way * (n // 2) + s - 1
        o = lax.rem(me + (s - 1) * (1 if way else -1) + n, n)
        sl = w2_part(axis, o, s, way, part)
        to = (zid if axis == 0 else yid)(-1 if way else 1)
        send(sl, sl, w2_s.at[axis, k, part], w2_r.at[axis, k, part], to)

    def w2_wait(axis, way, s, part):
        n, me = (zn, z) if axis == 0 else (yn, y)
        k = way * (n // 2) + s - 1
        o = lax.rem(me + s * (1 if way else -1) + n, n)
        sl = w2_part(axis, o, s, way, part)
        landed(sl, w2_s.at[axis, k, part], w2_r.at[axis, k, part])

    def hop(axis, g, start):
        m, me, pos = (yn, z, y) if axis == 0 else (zn, y, z)
        n = zn if axis == 0 else yn
        b = lax.rem(pos + g + m, m)
        for way in (0, 1):
            o = me if start else lax.rem(me + (1 if way else -1) + n, n)
            ref = wa.at[o, b] if axis == 0 else wb.at[b, o]
            ss, rs = b_s.at[axis, way, g % m], b_r.at[axis, way, g % m]
            if start:
                send(ref, ref, ss, rs, (zid if axis == 0 else yid)(-1 if way else 1))
            else:
                landed(ref, ss, rs)

    def w2_step(s, part):
        for axis, n in ((0, zn), (1, yn)):
            m = yn if axis == 0 else zn
            if s == 2 and part == 0:
                for g in range(m):
                    hop(axis, g, False)
            for way in (0, 1):
                if 2 < s <= n // 2 + 1:
                    w2_wait(axis, way, s - 1, part)
                if s <= n // 2:
                    w2_send(axis, way, s, part)

    for kind in (0, 1, 2):
        for axis in (0, 1):
            for way in (0, 1):
                ring(axis, way, 1, kind, True)
    hop(0, 0, True)
    hop(1, 0, True)

    def ring_step(s, kinds):
        for kind in kinds:
            for axis, n in ((0, yn), (1, zn)):
                for way in (0, 1):
                    if s <= n // 2:
                        ring(axis, way, s, kind, False)
                    if s + 1 <= n // 2:
                        ring(axis, way, s + 1, kind, True)

    ring_step(1, (0, 1))
    for i in range(1, yn):
        landed(gat.at[lax.rem(y - i + yn, yn)], gat_s.at[0, i], gat_r.at[0, i])
    before = jnp.zeros((8, tok), F32)
    for i in range(yn):
        block = gat[i]
        cums[i] = (before + block) * LOG2E
        before = before + jnp.broadcast_to(block[:, tok - 1 : tok], block.shape)
    gatz[z, 0:8] = cums[y]
    gatz[z, 8:16] = before * LOG2E
    for i in range(1, zn):
        send(gatz.at[z], gatz.at[z], gat_s.at[1, i], gat_r.at[1, i], zid(i))
    ring_step(1, (2,))
    for i in range(yn):
        for h in range(2):
            column = -jnp.broadcast_to(cums[i, h : h + 1, :], (tok, tok)).T
            biass[h, i * tok : (i + 1) * tok] = column
    for s in range(2, max(hy, hz) + 1):
        ring_step(s, (0, 1, 2))
        for axis, m in ((0, yn), (1, zn)):
            if s == 2 and m > 2:
                hop(axis, -1, True)
            if s == 3 and m > 2:
                hop(axis, 1, True)
                hop(axis, -2, True)
        if s == 2:
            for i in range(1, zn):
                landed(gatz.at[lax.rem(z - i + zn, zn)], gat_s.at[1, i], gat_r.at[1, i])
            gap = jnp.zeros((8, tok), F32)
            for i in reversed(range(zn)):
                gap = jnp.where(i < z, gap + gatz[i, 8:16], 0.0)
                away = jnp.where(i > z, -NEG, gatz[i, 2:3] - gap[2:3])
                column = -jnp.broadcast_to(away, (tok, tok)).T
                for j in range(2):
                    biasl[j, i * tok : (i + 1) * tok] = column
            edge[...] = -jnp.broadcast_to(gatz[z, 2:3], (tok, tok)).T

    for axis, m in ((0, yn), (1, zn)):
        for g in range(1, m):
            if g not in (1, m - 1, m - 2):
                hop(axis, g, True)
    key_lane = lax.broadcasted_iota(jnp.int32, (tok, 128), 1)
    for i in range(yn):
        rows = slice(i * tok, (i + 1) * tok)
        ksm = ty[i, 0]
        zero = jnp.zeros_like(ksm)
        kks[0, rows] = jnp.where(key_lane < 64, ksm, zero)
        kks[1, rows] = jnp.where(key_lane < 64, zero, ksm)
        vvs[:, rows] = ty[i, 1]
    for i in range(zn):
        rows = slice(i * tok, (i + 1) * tok)
        kkl[rows] = tz[i, 0]
        vvl[:, rows] = tz[i, 1]

    def soft(keys, queries, shifts, scale, values, limit):
        raw = nt(keys, queries)
        tops, dens, ps = [], [], []
        for j in range(2):
            s = raw[:, j * tok : (j + 1) * tok] * scale + shifts[j]
            if limit is not None and j == 0:
                spot = lax.broadcasted_iota(jnp.int32, s.shape, 0)
                s = jnp.where(spot <= limit, s, NEG)
            top = jnp.max(s, axis=0, keepdims=True)
            p = jnp.exp2(s - top)
            tops.append(top)
            dens.append(jnp.sum(p, axis=0, keepdims=True))
            ps.append(p.astype(BF16))
        return tops, dens, nn(values, jnp.concatenate(ps, axis=1))

    def two(ref, first_one, n):
        other = lax.rem(first_one + 1, n)
        return jnp.concatenate([ref[lax.rem(first_one, n), 2], ref[other, 2]], axis=0)

    def push(slot, i, to):
        rc(oout.at[slot, i], oin.at[slot, i], o_s.at[slot, i], o_r.at[slot, i], to).start()
        rc(sout.at[slot, i], sin.at[slot, i], st_s.at[slot, i], st_r.at[slot, i], to).start()

    def small(p, limit):
        queries = two(tz, z + 2 * p, zn)
        for h in range(2):
            lo, hi = 64 * h, 64 * h + 64
            shift = biass[h]
            tops, dens, part = soft(
                kks[h], queries, (shift, shift), 64 ** (-0.5) * LOG2E, vvs[lo:hi], limit
            )
            for j in range(2):
                piece = part[:, j * tok : (j + 1) * tok]
                if limit is not None and j == 0:
                    stats[0, h : h + 1] = tops[j]
                    stats[0, 2 + h : 3 + h] = dens[j]
                    accs[0, lo:hi] = piece
                else:
                    sout[0, 2 * p + j, h : h + 1] = tops[j]
                    sout[0, 2 * p + j, 2 + h : 3 + h] = dens[j]
                    oout[0, 2 * p + j, lo:hi] = piece.astype(BF16)
        for j in range(2):
            if limit is None or j == 1:

                @pl.when(z + 2 * p + j < zn)
                def _():
                    push(0, 2 * p + j, (sp + (2 * p + j) * yn, tp))

    def small_step(p, c):
        small(p, None)
        return c

    def large(p, c):
        a = lax.broadcasted_iota(jnp.int32, (tok, tok), 0)
        b = lax.broadcasted_iota(jnp.int32, (tok, tok), 1)
        rows = pl.ds(pl.multiple_of(z * tok, tok), tok)
        for j in range(2):
            o = lax.rem(y + 2 * p + j, yn)
            biasl[j, rows] = jnp.where(y * tok + a <= o * tok + b, edge[...], NEG)
        tops, dens, part = soft(
            kkl[...],
            two(ty, y + 2 * p, yn),
            (biasl[0], biasl[1]),
            128 ** (-0.5) * LOG2E,
            vvl[...],
            None,
        )
        for j in range(2):
            i = 2 * p + j
            o = lax.rem(y + i, yn)
            piece = part[:, j * tok : (j + 1) * tok]
            sout[1, i, 0:1] = tops[j]
            sout[1, i, 2:3] = dens[j]
            oout[1, i] = piece.astype(BF16)
            if j == 0:

                @pl.when(p == 0)
                def _():
                    statl[0, 0:1] = tops[0]
                    statl[0, 2:3] = dens[0]
                    accl[0] = piece

            @pl.when(jnp.logical_and(i > 0, jnp.logical_or(z > 0, o > y)))
            def _():
                push(1, i, (z * yn + o, tp))

        return c

    lax.fori_loop(0, yn // 2, large, 0)
    lax.fori_loop(1, (zn - z + 1) // 2, small_step, 0)
    small(0, y * tok + lax.broadcasted_iota(jnp.int32, (1, tok), 1))

    w2_step(2, 0)
    w2_step(2, 1)

    def fold(acc, stat, slot, lo, hi, i, row, gap):
        old = stat[0, row : row + 1]
        new = sin[slot, i, row : row + 1]
        if gap is not None:
            new = new + gap
        top = jnp.maximum(old, new)
        a = jnp.exp2(old - top)
        b = jnp.exp2(new - top)
        stat[0, row : row + 1] = top
        den = a * stat[0, 2 + row : 3 + row] + b * sin[slot, i, 2 + row : 3 + row]
        stat[0, 2 + row : 3 + row] = den
        acc[0, lo:hi] = a * acc[0, lo:hi] + b * oin[slot, i, lo:hi].astype(F32)

    def merge(i, gap):
        landed(oin.at[0, i], o_s.at[0, i], o_r.at[0, i])
        landed(sin.at[0, i], st_s.at[0, i], st_r.at[0, i])
        gap = gap + gatz[z - i, 8:16]
        for h in range(2):
            fold(accs, stats, 0, 64 * h, 64 * h + 64, i, h, gap[h : h + 1])
        return gap

    lax.fori_loop(1, z + 1, merge, jnp.zeros((8, tok), F32))

    def merge_large(i, c):
        @pl.when(jnp.logical_or(z > 0, lax.rem(y - i + yn, yn) < y))
        def _():
            landed(oin.at[1, i], o_s.at[1, i], o_r.at[1, i])
            landed(sin.at[1, i], st_s.at[1, i], st_r.at[1, i])
            fold(accl, statl, 1, 0, 128, i, 0, None)

        return c

    lax.fori_loop(1, yn, merge_large, 0)
    normed = []
    for h in range(3):
        if h < 2:
            att = accs[0, 64 * h : 64 * h + 64] / stats[0, 2 + h : 3 + h]
        else:
            att = accl[0] / statl[0, 2:3]
        mean = jnp.mean(att * att, axis=0, keepdims=True)
        normed.append(att * lax.rsqrt(mean + EPS))
    nsm = jnp.concatenate(normed[:2], axis=0).T.astype(BF16)
    nla = normed[2].T.astype(BF16)
    for c in loads[-2:]:
        c.wait()
    width = min(512, d)
    for c in range(d // width):
        cols = slice(c * width, (c + 1) * width)
        fpo[:, cols] = (nn(nsm, wos_ref[:, cols]) + nn(nla, wol_ref[:, cols])).astype(BF16)

    def mine(ref, t):
        return ref.at[pl.ds(pl.multiple_of(t * own, own), own)]

    for i in range(1, tn):
        send(mine(fpo, lax.rem(tp + i, tn)), fpi.at[i], fp_s.at[i], fp_r.at[i], tid(i))
    w2_step(3, 0)
    value = res_ref[...].astype(F32) + mine(fpo, tp)[...].astype(F32)
    for i in range(1, tn):
        landed(fpi.at[i], fp_s.at[i], fp_r.at[i])
        value = value + fpi[i].astype(F32)
    first[...] = value
    mean = jnp.mean(value * value, axis=1, keepdims=True)
    normal = value * lax.rsqrt(mean + EPS) * gain_ref[...]
    place = ext.at[pl.ds(pl.multiple_of(16 + tp * own, 16), own)]
    place[...] = normal.astype(BF16)
    for i in range(1, tn):
        send(place, place, n_s.at[i], n_r.at[i], tid(i))
    hw = d // 8

    @pl.when(jnp.logical_and(tp == tn - 1, sp < zn * yn - 1))
    def _():
        rows = [normal[own - 2 : own, c * hw : (c + 1) * hw] for c in range(8)]
        halo_out[...] = jnp.concatenate(rows, axis=0).astype(BF16)
        for i in range(tn):
            rc(halo_out, halo_in, h_s.at[i], h_r, (sp + 1, i)).start()

    w2_step(3, 1)
    w2_step(4, 0)

    @pl.when(sp > 0)
    def _():
        landed(halo_in, h_s.at[0], h_r)
        block = halo_in[...].astype(F32)
        for c in range(8):
            pad = jnp.zeros((14, hw), F32)
            rim = jnp.concatenate([pad, block[2 * c : 2 * c + 2]], axis=0)
            ext[0:16, c * hw : (c + 1) * hw] = rim.astype(BF16)

    for i in range(1, tn):
        src = lax.rem(tp - i + tn, tn)
        landed(ext.at[pl.ds(pl.multiple_of(16 + src * own, 16), own)], n_s.at[i], n_r.at[i])
    w2_step(4, 1)
    w2_step(5, 0)

    count = zn * yn
    for h, (w, _n) in enumerate(((wa, 0), (wb, 1))):
        cols = slice(h * half, (h + 1) * half)
        conv = []
        for j, taps in ((0, cg_ref), (1, cu_ref)):
            weight = w[:, :, j * wrows : (j + 1) * wrows].reshape(count * wrows, half)
            ebuf[j] = nn(ext[...], weight).astype(BF16).astype(F32)
            conv.append(
                taps[0:1, cols] * ebuf[j, 14 : 14 + tok]
                + taps[1:2, cols] * ebuf[j, 15 : 15 + tok]
                + taps[2:3, cols] * ebuf[j, 16 : 16 + tok]
            )
        hid[h] = (conv[0] / (1.0 + jnp.exp(-conv[0])) * conv[1]).astype(BF16)

    w2_step(5, 1)
    zs = max(1, zn // 4)
    for c in range(zn // zs):
        span = zs * yn * wrows
        total_down = None
        for h, w in enumerate((wa, wb)):
            weight = w[c * zs : (c + 1) * zs, :, 2 * wrows : 3 * wrows].reshape(span, half)
            term = nt(hid[h], weight)
            total_down = term if total_down is None else total_down + term
        dno[:, :, :, c * span : (c + 1) * span] = total_down.astype(BF16).reshape(
            tn // 2, 2, own, span
        )
    core = lax.rem(tp, 2)
    mate = (sp, tp + 1 - 2 * core)
    pairs = tn // 2
    spot = tp // 2
    send(dno.at[:, 1 - core], dnm, d_s.at[0], d_r.at[0], mate)
    landed(dnm, d_s.at[0], d_r.at[0])
    for i in range(1, pairs):
        k = lax.rem(spot + i, pairs)
        dnx[i] = (dno[k, core].astype(F32) + dnm[k].astype(F32)).astype(BF16)
        send(dnx.at[i], dni.at[i], d_s.at[i], d_r.at[i], (sp, 2 * k + core))
    value = first[...] + dno[spot, core].astype(F32) + dnm[spot].astype(F32)
    for i in range(1, pairs):
        landed(dni.at[i], d_s.at[i], d_r.at[i])
        value = value + dni[i].astype(F32)
    out_ref[...] = value

    for c in sends:
        c.wait_send()
    for i in range(1, zn):

        @pl.when(z + i < zn)
        def _():
            rc(oout.at[0, i], oin.at[0, i], o_s.at[0, i], o_r.at[0, i], yid(1)).wait_send()
            rc(sout.at[0, i], sin.at[0, i], st_s.at[0, i], st_r.at[0, i], yid(1)).wait_send()

    for i in range(1, yn):

        @pl.when(jnp.logical_or(z > 0, lax.rem(y + i, yn) > y))
        def _():
            rc(oout.at[1, i], oin.at[1, i], o_s.at[1, i], o_r.at[1, i], yid(1)).wait_send()
            rc(sout.at[1, i], sin.at[1, i], st_s.at[1, i], st_r.at[1, i], yid(1)).wait_send()

    @pl.when(jnp.logical_and(tp == tn - 1, sp < zn * yn - 1))
    def _():
        for i in range(tn):
            rc(halo_out, halo_in, h_s.at[i], h_r, yid(1)).wait_send()


def body(
    sizes,
    residual,
    q_small,
    k_small,
    v_small,
    q_large,
    k_large,
    v_large,
    forget_small,
    forget_large,
    w_out_small,
    w_out_large,
    norm_gain,
    w_gate,
    w_up,
    conv_gate,
    conv_up,
    w_down,
):
    zn, yn, tn = sizes
    tok = q_small.shape[0]
    own, d = residual.shape
    wrows, ff = w_gate.shape
    half = ff // 2
    operands = (
        residual,
        q_small,
        k_small,
        v_small,
        q_large,
        k_large,
        v_large,
        forget_small.T,
        forget_large.T,
        w_out_small,
        w_out_large,
        norm_gain.reshape(1, d),
        w_gate,
        w_up,
        conv_gate,
        conv_up,
        w_down.T,
    )
    dma = pltpu.SemaphoreType.DMA
    big = max(yn, zn)
    scratch = [
        *(pltpu.VMEM(a.shape, a.dtype) for a in operands),
        pltpu.VMEM((yn, 8, tok), F32),
        pltpu.VMEM((zn, 16, tok), F32),
        pltpu.VMEM((yn, 3, tok, 128), BF16),
        pltpu.VMEM((zn, 3, tok, 128), BF16),
        pltpu.VMEM((zn, yn, 3 * wrows, half), BF16),
        pltpu.VMEM((zn, yn, 3 * wrows, half), BF16),
        pltpu.VMEM((yn, 8, tok), F32),
        pltpu.VMEM((2, yn * tok, tok), F32),
        pltpu.VMEM((2, zn * tok, tok), F32),
        pltpu.VMEM((tok, tok), F32),
        pltpu.VMEM((2, yn * tok, 128), BF16),
        pltpu.VMEM((zn * tok, 128), BF16),
        pltpu.VMEM((128, yn * tok), BF16),
        pltpu.VMEM((128, zn * tok), BF16),
        pltpu.VMEM((1, 128, tok), F32),
        pltpu.VMEM((1, 128, tok), F32),
        pltpu.VMEM((1, 8, tok), F32),
        pltpu.VMEM((1, 8, tok), F32),
        pltpu.VMEM((2, big, 128, tok), BF16),
        pltpu.VMEM((2, big, 128, tok), BF16),
        pltpu.VMEM((2, big, 8, tok), F32),
        pltpu.VMEM((2, big, 8, tok), F32),
        pltpu.VMEM((tok, d), BF16),
        pltpu.VMEM((tn, own, d), BF16),
        pltpu.VMEM((tn // 2, 2, own, d), BF16),
        pltpu.VMEM((tn // 2, own, d), BF16),
        pltpu.VMEM((tn // 2, own, d), BF16),
        pltpu.VMEM((tn // 2, own, d), BF16),
        pltpu.VMEM((own, d), F32),
        pltpu.VMEM((tok + 16, d), BF16),
        pltpu.VMEM((16, d // 8), BF16),
        pltpu.VMEM((16, d // 8), BF16),
        pltpu.VMEM((2, tok + 16, half), F32),
        pltpu.VMEM((2, tok, half), BF16),
        dma((len(operands),)),
        dma((2, big)),
        dma((2, big)),
        dma((2, big, 2)),
        dma((2, big, 2)),
        dma((2, big)),
        dma((2, big)),
        dma((2, 2, big)),
        dma((2, 2, big)),
        dma((2, big, 2)),
        dma((2, big, 2)),
        dma((2, big)),
        dma((2, big)),
        dma((2, big)),
        dma((2, big)),
        dma((tn,)),
        dma((tn,)),
        dma((tn,)),
        dma((tn,)),
        dma((tn,)),
        dma((tn,)),
        dma((tn,)),
        dma,
    ]
    vmem = pl.BlockSpec(memory_space=pltpu.VMEM)
    hbm = pl.BlockSpec(memory_space=pl.ANY)
    result = pl.pallas_call(
        functools.partial(kernel, zn, yn, tn),
        out_shape=pltpu.VMEM((own, d), F32),
        in_specs=[hbm] * len(operands),
        out_specs=pl.BlockSpec(memory_space=pltpu.VMEM),
        scratch_shapes=scratch,
        compiler_params=pltpu.CompilerParams(
            collective_id=0, has_side_effects=True, vmem_limit_bytes=60 * 1024 * 1024
        ),
    )(*operands)
    return result.astype(BF16)


def solution(mesh):
    sp = mesh.shape["sp"]
    yn = math.isqrt(sp)
    zn = sp // yn
    placed = (
        P(("sp", "tp"), None),
        P("sp", "tp"),
        P("sp", "tp"),
        P("sp", "tp"),
        P("sp", "tp"),
        P("sp", "tp"),
        P("sp", "tp"),
        P("sp", "tp"),
        P("sp", "tp"),
        P("tp", None),
        P("tp", None),
        P(),
        P("sp", "tp"),
        P("sp", "tp"),
        P(None, "tp"),
        P(None, "tp"),
        P("tp", "sp"),
    )
    return jax.shard_map(
        functools.partial(body, (zn, yn, mesh.shape["tp"])),
        mesh=mesh,
        in_specs=placed,
        out_specs=P(("sp", "tp"), None),
        check_vma=False,
    )
```
